32 devices in a mesh: rep: 2 (over x), fs: 8 (over z, y), tp: 2 (over core).
Axes of the slice: x: 2, y: 2, z: 4, core: 2. Of those that a mesh axis runs over, the one named last changes fastest.
Arguments:
- resid: bfloat16 [12288, 2048], P(('rep', 'fs', 'tp')), may hold values from -6 to 6
- mix_gain: float32 [2048], replicated, may hold values from 0.1 to 1.9
- query_weight: bfloat16 [2048, 1024], P('fs', 'tp'), may hold values from -0.125 to 0.125
- key_weight: bfloat16 [2048, 1024], P('fs', 'tp'), may hold values from -0.125 to 0.125
- value_weight: bfloat16 [2048, 2048], P('fs', 'tp'), may hold values from -0.125 to 0.125
- head_gain: float32 [2048], P('tp'), may hold values from 0.1 to 1.9
- out_weight: bfloat16 [2048, 2048], P('tp', 'fs'), may hold values from -0.125 to 0.125
- mlp_gain: float32 [2048], replicated, may hold values from 0.1 to 1.9
- gate_weight: bfloat16 [2048, 2816], P('fs', 'tp'), may hold values from -0.125 to 0.125
- up_weight: bfloat16 [2048, 2816], P('fs', 'tp'), may hold values from -0.125 to 0.125
- down_weight: bfloat16 [2816, 2048], P('tp', 'fs'), may hold values from -0.109375 to 0.109375
Outputs:
- layer_out: bfloat16 [12288, 2048], P(('rep', 'fs', 'tp'))
The draws below stay inside these ranges and needn't reach their ends.
All inputs are finite; a program needn't handle non-finite values.
Results may differ from the reference program's by a relative error of at most 0.014.
Values may be sent and summed in bfloat16 or wider, within the bound.
A program may use at most 128 MiB of HBM per device.

```python
import jax
import jax.numpy as jnp
from jax import lax

D = 2048
HEADS = 4
DK = 256
DV = 512
FF = 2816
BLOCK = 128
LEN = 768
TOKENS = 12288
N_TP = 2


def shard_levels(own_key, shape, pieces, least, top_value):
    def one(dim, parts):
        heights = jax.random.uniform(jax.random.fold_in(jax.random.fold_in(own_key, 6), dim), (parts,), jnp.float32, least / len(pieces), top_value / len(pieces))
        return jnp.repeat(jnp.exp(heights), shape[dim] // parts).reshape((-1,) + (1,) * (len(shape) - dim - 1))

    level = one(*pieces[0])
    for cut in pieces[1:]:
        level = level * one(*cut)
    return level


def noise(stream_key, dims, spread, reach, split=(), held_as=jnp.bfloat16):
    level = shard_levels(stream_key, dims, split, -0.22, 0.18) if split else 1.0
    entries = jax.random.normal(stream_key, dims, jnp.float32) * spread * level
    return jnp.minimum(jnp.maximum(entries, -reach), reach).astype(held_as)


def setup_inputs(seed: int = 0) -> dict:
    arg_keys = jax.random.split(jax.random.key(seed), 12)
    resid = noise(arg_keys[0], (TOKENS, D), 1.0, 6.0, ((0, 32),))
    mix_gain = jnp.clip(1.0 + 0.18 * jax.random.normal(arg_keys[1], (D,), jnp.float32), 0.1, 1.9)
    query_weight = noise(arg_keys[2], (D, HEADS * DK), D ** -0.5, 0.125, ((0, 8), (1, 2)))
    key_weight = noise(arg_keys[3], (D, HEADS * DK), D ** -0.5, 0.125, ((0, 8), (1, 2)))
    value_weight = noise(arg_keys[4], (D, HEADS * DV), D ** -0.5, 0.125, ((0, 8), (1, 2)))
    head_gain = jnp.clip(1.0 + 0.18 * jax.random.normal(arg_keys[5], (HEADS * DV,), jnp.float32), 0.1, 1.9)
    out_weight = noise(arg_keys[6], (HEADS * DV, D), (HEADS * DV) ** -0.5, 0.125, ((0, 2), (1, 8)))
    mlp_gain = jnp.clip(1.0 + 0.18 * jax.random.normal(arg_keys[7], (D,), jnp.float32), 0.1, 1.9)
    gate_weight = noise(arg_keys[8], (D, FF), D ** -0.5, 0.125, ((0, 8), (1, 2)))
    up_weight = noise(arg_keys[9], (D, FF), D ** -0.5, 0.125, ((0, 8), (1, 2)))
    down_weight = noise(arg_keys[10], (FF, D), FF ** -0.5, 0.109375, ((0, 2), (1, 8)))
    return {"resid": resid, "mix_gain": mix_gain, "query_weight": query_weight, "key_weight": key_weight, "value_weight": value_weight, "head_gain": head_gain, "out_weight": out_weight, "mlp_gain": mlp_gain, "gate_weight": gate_weight, "up_weight": up_weight, "down_weight": down_weight}


norm_eps = 1e-06
rope_base = 10000.0

def stored(values):
    return lax.optimization_barrier(values.astype(jnp.bfloat16)).astype(jnp.float32)

def rms_scale(values, gain):
    widened = values.astype(jnp.float32)
    scaled = widened * lax.rsqrt(lax.optimization_barrier(jnp.mean(widened * widened, axis=-1, keepdims=True)) + norm_eps)
    return (scaled * gain.astype(jnp.float32)).astype(jnp.bfloat16)

def rotate(vectors):
    length_total = vectors.shape[0]
    half_width = vectors.shape[-1] // 2
    position = jnp.arange(length_total, dtype=jnp.float32)
    inverse = 1.0 / rope_base ** jnp.linspace(0.0, 1.0, half_width, dtype=jnp.float32)
    angle = position[:, None] * inverse[None, :]
    cosine = jnp.cos(angle)[:, None, :]
    sine = jnp.sin(angle)[:, None, :]
    first = vectors[..., :half_width]
    second = vectors[..., half_width:]
    return jnp.concatenate([first * cosine - second * sine, second * cosine + first * sine], axis=-1)

def decay_tables(head_ids, block):
    log_gamma = jnp.log1p(-2.0 ** (-5.0 - 2.0 * head_ids.astype(jnp.float32)))
    offset = jnp.arange(block, dtype=jnp.float32)
    distance = offset[:, None] - offset[None, :]
    inside = jnp.where(distance >= 0, jnp.exp(log_gamma[:, None, None] * jnp.maximum(distance, 0.0)), 0.0)
    query_decay = jnp.exp(log_gamma[:, None] * (offset + 1.0))
    key_decay = jnp.exp(log_gamma[:, None] * (block - 1.0 - offset))
    block_decay = jnp.exp(log_gamma * block)
    return (inside, query_decay, key_decay, block_decay)

def retain(queries, keys, values, head_ids, block):
    length_total, heads, key_width = queries.shape
    value_width = values.shape[-1]
    count = length_total // block
    inside, query_decay, key_decay, block_decay = decay_tables(head_ids, block)

    def blocks(tensor):
        return tensor.reshape(count, block, heads, tensor.shape[-1]).transpose(0, 2, 1, 3)

    def advance(memory, inputs):
        query_tile_rows, key_tile_rows, value_block = inputs
        query_widened = query_tile_rows.astype(jnp.float32)
        value_wide = value_block.astype(jnp.float32)
        attention_scores = jnp.einsum('zvf,zjf->zvj', query_widened, key_tile_rows.astype(jnp.float32))
        weights = stored(attention_scores * inside)
        within = jnp.einsum('hlm,hmv->hlv', weights, value_wide)
        carried = jnp.einsum('hld,hdv->hlv', query_widened, stored(memory)) * query_decay[:, :, None]
        weighted_keys = stored(key_tile_rows.astype(jnp.float32) * key_decay[:, :, None])
        memory = memory * block_decay[:, None, None] + jnp.einsum('hld,hlv->hdv', weighted_keys, value_wide)
        return (memory, within + carried)
    start_state = jnp.zeros((heads, key_width, value_width), jnp.float32)
    _, outputs = lax.scan(advance, start_state, (blocks(queries), blocks(keys), blocks(values)))
    return outputs.transpose(0, 2, 1, 3).reshape(length_total, heads, value_width)

def head_scale(retained, gain):
    scaled = retained * lax.rsqrt(lax.optimization_barrier(jnp.mean(retained * retained, axis=-1, keepdims=True)) + norm_eps)
    return (scaled.reshape(retained.shape[0], -1) * gain.astype(jnp.float32)).astype(jnp.bfloat16)

def reference(resid, mix_gain, query_weight, key_weight, value_weight, head_gain, out_weight, mlp_gain, gate_weight, up_weight, down_weight):
    head_ids = jnp.arange(HEADS, dtype=jnp.int32)
    head_share = HEADS * DV // N_TP
    unit_share = FF // N_TP

    def single_sequence(token_rows):
        normed = rms_scale(token_rows, mix_gain)
        queries = stored(jnp.dot(normed, query_weight, preferred_element_type=jnp.float32)).reshape(LEN, HEADS, DK)
        keys = stored(jnp.dot(normed, key_weight, preferred_element_type=jnp.float32)).reshape(LEN, HEADS, DK)
        values = jnp.dot(normed, value_weight, preferred_element_type=jnp.float32).astype(jnp.bfloat16)
        values = values.reshape(LEN, HEADS, DV)
        query_rot = rotate(queries).astype(jnp.bfloat16)
        key_rot = (rotate(keys) * DK ** (-0.5)).astype(jnp.bfloat16)
        retained = retain(query_rot, key_rot, values, head_ids, BLOCK)
        head_out = head_scale(retained, head_gain)
        mixer_sum = jnp.zeros((LEN, D), jnp.float32)
        for group in range(N_TP):
            lower = group * head_share
            partial_sum = jnp.dot(head_out[:, lower:lower + head_share], out_weight[lower:lower + head_share], preferred_element_type=jnp.float32)
            mixer_sum = mixer_sum + stored(partial_sum)
        middle = (token_rows.astype(jnp.float32) + mixer_sum).astype(jnp.bfloat16)
        normed_mlp = rms_scale(middle, mlp_gain)
        gate = jnp.dot(normed_mlp, gate_weight, preferred_element_type=jnp.float32)
        upward = jnp.dot(normed_mlp, up_weight, preferred_element_type=jnp.float32)
        hidden_units = (jax.nn.silu(gate) * upward).astype(jnp.bfloat16)
        mlp_sum = jnp.zeros((LEN, D), jnp.float32)
        for group in range(N_TP):
            lower = group * unit_share
            partial_sum = jnp.dot(hidden_units[:, lower:lower + unit_share], down_weight[lower:lower + unit_share], preferred_element_type=jnp.float32)
            mlp_sum = mlp_sum + stored(partial_sum)
        return (middle.astype(jnp.float32) + mlp_sum).astype(jnp.bfloat16)
    sequences = resid.reshape(TOKENS // LEN, LEN, D)
    return lax.map(single_sequence, sequences).reshape(TOKENS, D)
```

```python
import functools
import math

import jax
import jax.numpy as jnp
import numpy as np
from jax import lax
from jax.experimental import pallas as pl
from jax.experimental.pallas import tpu as pltpu
from jax.sharding import PartitionSpec as P

UNITS = 8
MESH = pl.DeviceIdType.MESH


class Stream:
    def __init__(self, w, first, count, along_z, along_y):
        self.w, self.first, self.count = w, first, count
        self.along_z, self.along_y = along_z, along_y


class Exchange:
    def __init__(self, depth, streams, shapes, axes, fulls, send_sem, recv_sem):
        self.depth, self.streams = depth, streams
        self.shapes, self.axes, self.fulls = shapes, axes, fulls
        self.send_sem, self.recv_sem = send_sem, recv_sem
        self.x = lax.axis_index("rep")
        fs = lax.axis_index("fs")
        self.z = fs // 2
        self.y = lax.rem(fs, 2)

    def barrier(self):
        sem = pltpu.get_barrier_semaphore()
        z, y, x = self.z, self.y, self.x
        core = lax.axis_index("tp")
        pl.semaphore_signal(sem, inc=1, device_id={"tp": 1 - core}, device_id_type=MESH)
        pl.semaphore_signal(sem, inc=1, device_id={"rep": 1 - x}, device_id_type=MESH)
        pl.semaphore_signal(sem, inc=1, device_id={"fs": z * 2 + 1 - y}, device_id_type=MESH)

        @pl.when(z > 0)
        def _():
            pl.semaphore_signal(sem, inc=1, device_id={"fs": (z - 1) * 2 + y}, device_id_type=MESH)

        @pl.when(z < self.depth - 1)
        def _():
            pl.semaphore_signal(sem, inc=1, device_id={"fs": (z + 1) * 2 + y}, device_id_type=MESH)

        low = jnp.minimum(z, 1)
        high = jnp.minimum(self.depth - 1 - z, 1)
        pl.semaphore_wait(sem, 3 + low + high)

    def slot(self, w, block, start, count):
        rows, cols = self.shapes[w]
        if self.axes[w] == 0:
            first = pl.multiple_of(block * rows + start, 16)
            return self.fulls[w].at[pl.ds(first, count), :]
        return self.fulls[w].at[
            pl.ds(pl.multiple_of(start, 16), count), pl.ds(pl.multiple_of(block * cols, 128), cols)
        ]

    def copy(self, s, kind, origin, incoming=False):
        stream = self.streams[s]
        x, y, z = self.x, self.y, self.z
        a, b = stream.along_z, stream.along_y
        unit = stream.count // UNITS
        xs = 1 - x if incoming and kind in ("x1", "x2") else x
        start, count = {
            "up": ((UNITS - a) * x, a),
            "down": ((UNITS - a) * x, a),
            "y": ((UNITS - b) * x, b),
            "x1": (a * xs, UNITS - a),
            "x2": (b * xs, UNITS - b),
        }[kind]
        start, count = stream.first + start * unit, count * unit
        far = kind == "x2" or (incoming and kind == "y")
        block = origin * 2 + (1 - y if far else y)
        target = {
            "up": {"fs": (z + 1) * 2 + y},
            "down": {"fs": (z - 1) * 2 + y},
            "y": {"fs": z * 2 + 1 - y},
            "x1": {"rep": 1 - x},
            "x2": {"rep": 1 - x},
        }[kind]
        place = self.slot(stream.w, block, start, count)
        sends = ("up", "down", "y", "x1", "x2").index(kind)
        receives = (0, 0, 1, 2, 3)[sends]
        return pltpu.make_async_remote_copy(
            src_ref=place,
            dst_ref=place,
            send_sem=self.send_sem.at[s, sends, origin],
            recv_sem=self.recv_sem.at[s, receives, origin],
            device_id=target,
            device_id_type=MESH,
        )

    def each(self, t, body):
        if t == 0:
            body("own", self.z)
            return

        @pl.when(self.z - t >= 0)
        def _():
            body("up", self.z - t)

        @pl.when(self.z + t < self.depth)
        def _():
            body("down", self.z + t)

    def onward(self, s, way, origin, act):
        if way in ("own", "up"):

            @pl.when(self.z < self.depth - 1)
            def _():
                act(self.copy(s, "up", origin))

        if way in ("own", "down"):

            @pl.when(self.z > 0)
            def _():
                act(self.copy(s, "down", origin))

    def step(self, s, t):
        if t < self.depth:

            def arrive(way, origin):
                if way != "own":
                    self.copy(s, way, origin, incoming=True).wait_recv()
                self.onward(s, way, origin, lambda c: c.start())
                self.copy(s, "y", origin).start()
                if way != "own":
                    self.copy(s, "x1", origin).start()

            self.each(t, arrive)
        if 1 <= t <= self.depth:

            def cross(way, origin):
                self.copy(s, "y", origin, incoming=True).wait_recv()
                self.copy(s, "x2", origin).start()

            self.each(t - 1, cross)
        if t == self.depth + 1:
            for back in range(self.depth):

                def last(way, origin):
                    if way != "own":
                        self.copy(s, "x1", origin, incoming=True).wait_recv()
                    self.copy(s, "x2", origin, incoming=True).wait_recv()

                self.each(back, last)

    def drain(self, s):
        for back in range(self.depth):

            def sent(way, origin):
                self.onward(s, way, origin, lambda c: c.wait_send())
                self.copy(s, "y", origin).wait_send()
                if way != "own":
                    self.copy(s, "x1", origin).wait_send()
                self.copy(s, "x2", origin).wait_send()

            self.each(back, sent)


class Peer:
    def __init__(self, send_sem, recv_sem):
        self.send_sem, self.recv_sem = send_sem, recv_sem
        self.core = lax.axis_index("tp")

    def copy(self, index, source, place):
        return pltpu.make_async_remote_copy(
            src_ref=source,
            dst_ref=place,
            send_sem=self.send_sem.at[index],
            recv_sem=self.recv_sem.at[index],
            device_id={"tp": 1 - self.core},
            device_id_type=MESH,
        )


def rotated(v, cosine, sine):
    half = v.shape[-1] // 2
    first, second = v[:, :half], v[:, half:]
    return jnp.concatenate(
        [first * cosine - second * sine, second * cosine + first * sine], axis=-1
    )


def column_dot(left, right, out, first, last, width=256):
    @pl.loop(first, last)
    def _(c):
        cols = pl.ds(pl.multiple_of(c * width, width), width)
        out[:, cols] = jnp.dot(
            left[...], right[:, cols], preferred_element_type=jnp.float32
        ).astype(out.dtype)


def scaled_rows(values, gain):
    scale = lax.rsqrt(jnp.mean(values * values, axis=-1, keepdims=True) + norm_eps)
    return (values * scale * gain).astype(jnp.bfloat16)


def decay_rates(ids):
    return [math.log1p(-(2.0 ** (-5.0 - 2.0 * i))) for i in ids]


def make_tables(heads, inside, query_decay, key_decay):
    core = lax.axis_index("tp")
    block = inside.shape[-1]
    rates = decay_rates(range(2 * heads))
    row = lax.broadcasted_iota(jnp.int32, (block, block), 0).astype(jnp.float32)
    col = lax.broadcasted_iota(jnp.int32, (block, block), 1).astype(jnp.float32)
    distance = row - col
    for h in range(heads):
        rate = jnp.where(core == 0, rates[h], rates[heads + h])
        inside[h] = jnp.where(
            distance >= 0, jnp.exp(rate * jnp.maximum(distance, 0.0)), 0.0
        )
        query_decay[h] = jnp.exp(rate * (row + 1.0))
        key_decay[h] = jnp.exp(rate * (block - 1.0 - row))


def retain_blocks(h, heads, first, last, tables, proj, memory, head_out):
    cos_ref, sin_ref, inside, query_decay, key_decay, gain = tables
    core = lax.axis_index("tp")
    block = inside.shape[-1]
    rates = decay_rates(range(2 * heads))
    block_decay = jnp.where(
        core == 0, math.exp(rates[h] * block), math.exp(rates[heads + h] * block)
    )
    if first == 0:
        memory[...] = jnp.zeros_like(memory)
    q_cols = pl.ds(h * DK, DK)
    k_cols = pl.ds((heads + h) * DK, DK)
    v_cols = pl.ds(2 * heads * DK + h * DV, DV)

    @pl.loop(first, last)
    def _(b):
        rows = pl.ds(pl.multiple_of(b * block, block), block)
        cosine, sine = cos_ref[rows, :], sin_ref[rows, :]
        q = rotated(proj[rows, q_cols].astype(jnp.float32), cosine, sine).astype(jnp.bfloat16)
        k = rotated(proj[rows, k_cols].astype(jnp.float32), cosine, sine) * DK ** (-0.5)
        k = k.astype(jnp.bfloat16)
        v = proj[rows, v_cols]
        scores = lax.dot_general(
            q, k, (((1,), (1,)), ((), ())), preferred_element_type=jnp.float32
        )
        weights = (scores * inside[h]).astype(jnp.bfloat16)
        state = memory[...]
        kept = jnp.dot(weights, v, preferred_element_type=jnp.float32) + query_decay[h][
            :, 0:1
        ] * jnp.dot(q, state.astype(jnp.bfloat16), preferred_element_type=jnp.float32)
        decayed = (k.astype(jnp.float32) * key_decay[h][:, 0:1]).astype(jnp.bfloat16)
        memory[...] = state * block_decay + lax.dot_general(
            decayed, v, (((0,), (0,)), ((), ())), preferred_element_type=jnp.float32
        )
        scale = lax.rsqrt(jnp.mean(kept * kept, axis=-1, keepdims=True) + norm_eps)
        head_out[rows, pl.ds(h * DV, DV)] = (
            kept * scale * gain[:, pl.ds(h * DV, DV)]
        ).astype(jnp.bfloat16)


ROWS = 64
WIDE = 512


def layer_kernel(depth, streams, shapes, heads, *refs):
    args, refs = refs[:13], refs[13:]
    resid, mix_gain, query, key, value, head_gain, out_w, mlp_gain, gate, up, down, cos, sin = args
    out, refs = refs[0], refs[1:]
    fulls, refs = refs[:4], refs[4:]
    mixer, out_full, mlp, down_full = fulls
    held, refs = refs[:6], refs[6:]
    x, gain_mix, gain_head, gain_mlp, cos_v, sin_v = held
    normed, both, proj, memory, head_out, hidden, part, sent, got, middle, result, refs = (
        *refs[:11],
        refs[11:],
    )
    inside, query_decay, key_decay, refs = *refs[:3], refs[3:]
    send_sem, recv_sem, load_sem, peer_send, peer_recv, out_sem = refs
    ex = Exchange(depth, streams, shapes, (0, 1, 0, 1), fulls, send_sem, recv_sem)
    peer = Peer(peer_send, peer_recv)
    core = lax.axis_index("tp")
    fs = lax.axis_index("fs")
    rows = x.shape[0]
    qc, kc, vc = query.shape[1], key.shape[1], value.shape[1]
    units = gate.shape[1]

    mixer_own = pl.ds(pl.multiple_of(fs * shapes[0][0], 16), shapes[0][0])
    mlp_own = pl.ds(pl.multiple_of(fs * shapes[2][0], 16), shapes[2][0])
    pairs = [
        (query, mixer.at[mixer_own, pl.ds(0, qc)]),
        (key, mixer.at[mixer_own, pl.ds(qc, kc)]),
        (value, mixer.at[mixer_own, pl.ds(qc + kc, vc)]),
        (out_w, ex.slot(1, fs, 0, shapes[1][0])),
        (resid, x),
        (mix_gain, gain_mix),
        (down, ex.slot(3, fs, 0, shapes[3][0])),
        (cos, cos_v),
        (sin, sin_v),
        (head_gain, gain_head),
        (mlp_gain, gain_mlp),
    ]
    loads = [
        pltpu.make_async_copy(source, place, load_sem.at[i])
        for i, (source, place) in enumerate(pairs)
    ]
    for load in loads[:6]:
        load.start()

    @pl.loop(0, units // 128)
    def _(j):
        cols = pl.ds(pl.multiple_of(j * 128, 128), 128)
        for i, source in enumerate((gate, up)):
            place = pl.ds(pl.multiple_of(j * 256, 128) + i * 128, 128)
            pltpu.make_async_copy(
                source.at[:, cols], mlp.at[mlp_own, place], load_sem.at[len(pairs)]
            ).start()

    for load in loads[6:]:
        load.start()
    mlp_slot = ex.slot(2, fs, 0, shapes[2][0])
    mlp_load = pltpu.make_async_copy(mlp_slot, mlp_slot, load_sem.at[len(pairs)])

    ex.barrier()

    own = pl.ds(pl.multiple_of(core * rows, 16), rows)
    other = pl.ds(pl.multiple_of((1 - core) * rows, 16), rows)
    join_mix = peer.copy(0, normed.at[own, :], normed.at[own, :])
    join_mlp = peer.copy(1, both.at[own, :], both.at[own, :])

    def norm_mix():
        loads[4].wait()
        loads[5].wait()

        @pl.loop(0, rows // ROWS)
        def _(r):
            here = pl.ds(pl.multiple_of(r * ROWS, ROWS), ROWS)
            there = pl.ds(pl.multiple_of(core * rows + r * ROWS, ROWS), ROWS)
            normed[there, :] = scaled_rows(x[here, :].astype(jnp.float32), gain_mix[...])

        join_mix.start()
        make_tables(heads, inside, query_decay, key_decay)
        for load in loads[7:]:
            load.wait()

    def share(index, c):
        cols = pl.ds(c * WIDE, WIDE)
        return peer.copy(index + c, sent.at[:, cols], got.at[:, cols])

    chunks = part.shape[1] // WIDE

    def product(left, right, index):
        for c in range(chunks):

            @pl.loop(0, WIDE // 256)
            def _(i):
                cols = pl.ds(pl.multiple_of(c * WIDE + i * 256, 256), 256)
                sent[:, cols] = jnp.dot(
                    left[other, :], right[:, cols], preferred_element_type=jnp.float32
                ).astype(jnp.bfloat16)

            share(index, c).start()
        for c in range(chunks):

            @pl.loop(0, WIDE // 256)
            def _(i):
                cols = pl.ds(pl.multiple_of(c * WIDE + i * 256, 256), 256)
                part[:, cols] = jnp.dot(
                    left[own, :], right[:, cols], preferred_element_type=jnp.float32
                ).astype(jnp.bfloat16)

    def norm_mlp():
        for c in range(chunks):
            share(2, c).wait()

        @pl.loop(0, rows // ROWS)
        def _(r):
            here = pl.ds(pl.multiple_of(r * ROWS, ROWS), ROWS)
            there = pl.ds(pl.multiple_of(core * rows + r * ROWS, ROWS), ROWS)
            total = part[here, :].astype(jnp.float32) + got[here, :].astype(jnp.float32)
            mid = (x[here, :].astype(jnp.float32) + total).astype(jnp.bfloat16)
            middle[here, :] = mid
            both[there, :] = scaled_rows(mid.astype(jnp.float32), gain_mlp[...])

        join_mlp.start()

    def expand():
        @pl.loop(0, units // 128)
        def _(j):
            cols = pl.ds(pl.multiple_of(j * 256, 256), 256)
            pair = jnp.dot(both[...], mlp[:, cols], preferred_element_type=jnp.float32)
            place = pl.ds(pl.multiple_of(j * 128, 128), 128)
            hidden[:, place] = (jax.nn.silu(pair[:, :128]) * pair[:, 128:]).astype(jnp.bfloat16)

    def finish():
        writes = []
        for c in range(chunks):
            cols = pl.ds(c * WIDE, WIDE)
            share(2 + chunks, c).wait()
            total = part[:, cols].astype(jnp.float32) + got2(cols)
            result[:, cols] = (middle[:, cols].astype(jnp.float32) + total).astype(jnp.bfloat16)
            write = pltpu.make_async_copy(result.at[:, cols], out.at[:, cols], out_sem.at[c])
            write.start()
            writes.append(write)
        for write in writes:
            write.wait()

    def got2(cols):
        return got[:, cols].astype(jnp.float32)

    blocks = proj.shape[0] // inside.shape[-1]
    tables = (cos_v, sin_v, inside, query_decay, key_decay, gain_head)
    columns = proj.shape[1] // 256
    plan = {0: [norm_mix]}
    span = 2 * (depth + 2) - 6
    half = blocks // 2
    first = 2 * (depth + 1) + 1

    def project(low, high):
        if low == 0:
            join_mix.wait()
        column_dot(normed, mixer, proj, low, high)

    plan[first] = [lambda: project(0, columns // 2)]
    plan[first + 1] = [lambda: project(columns // 2, columns)]
    at = first + 2
    for h in range(heads):
        for low, high in ((0, half), (half, blocks)):
            plan.setdefault(at, []).append(
                functools.partial(
                    retain_blocks, h, heads, low, high, tables, proj, memory, head_out
                )
            )
            at += 1
    plan.setdefault(first + 6, []).append(lambda: product(head_out, out_full, 2))
    plan.setdefault(first + 7, []).append(norm_mlp)

    def mlp_in():
        join_mlp.wait()
        expand()

    plan.setdefault(first + 12, []).append(mlp_in)
    plan.setdefault(first + 18, []).append(lambda: product(hidden, down_full, 2 + chunks))
    plan[first + 18].append(finish)
    count = len(streams)
    begin = {0: loads[:3], 2: loads[3:4], 4: [mlp_load], 6: loads[6:7]}
    for tick in range(first + 19):
        for s in range(count):
            t, odd = divmod(tick - 6 * (s // 2), 2)
            if odd == s % 2 and 0 <= t <= depth + 1:
                if t == 0:
                    for load in begin.get(s, ()):
                        load.wait()
                ex.step(s, t)
        for job in plan.get(tick, ()):
            job()
    for s in range(count):
        ex.drain(s)


def cut(total):
    whole = total // (UNITS * 16)
    first = (whole + 1) // 2 * UNITS * 16
    return first, total - first


def plan_streams(shapes):
    streams = []
    for w, (rows, _) in enumerate(shapes):
        first, second = cut(rows)
        streams.append(Stream(w, 0, first, 6, 5))
        streams.append(Stream(w, first, second, 7, 4))
    return streams


def rotation_tables(length_total, half_width):
    position = np.arange(length_total, dtype=np.float32)
    inverse = (1.0 / rope_base ** np.linspace(0.0, 1.0, half_width)).astype(np.float32)
    angle = (position[:, None] * inverse[None, :]).astype(np.float64)
    return np.cos(angle).astype(np.float32), np.sin(angle).astype(np.float32)


def fits(shapes, rows, heads):
    whole = all(r % (UNITS * 16) == 0 and r >= 2 * UNITS * 16 and c % 128 == 0 for r, c in shapes)
    sizes = lax.axis_size("rep") == 2 and lax.axis_size("fs") == 8 and lax.axis_size("tp") == 2
    return whole and sizes and rows % BLOCK == 0 and heads == 2


def layer(args, shapes, heads):
    resid, query, key, value, gate = args[0], args[2], args[3], args[4], args[8]
    size = lax.axis_size("fs")
    depth = size // 2
    rows, width = resid.shape
    length_total = 2 * rows
    streams = plan_streams(shapes)
    count = len(streams)
    fulls = []
    for (r, c), axis in zip(shapes, (0, 1, 0, 1)):
        fulls.append((r * size, c) if axis == 0 else (r, c * size))
    cosine, sine = rotation_tables(length_total, DK // 2)
    far = pl.BlockSpec(memory_space=pl.ANY)
    bf, f32 = jnp.bfloat16, jnp.float32
    vm = pltpu.VMEM
    dma = pltpu.SemaphoreType.DMA
    chunks = width // WIDE
    args = [a[None, :] if a.ndim == 1 else a for a in args]
    return pl.pallas_call(
        functools.partial(layer_kernel, depth, streams, shapes, heads),
        out_shape=jax.ShapeDtypeStruct((rows, width), bf),
        in_specs=[far] * 13,
        out_specs=far,
        scratch_shapes=[vm(s, bf) for s in fulls]
        + [
            vm((rows, width), bf),
            vm(args[1].shape, f32),
            vm(args[5].shape, f32),
            vm(args[7].shape, f32),
            vm(cosine.shape, f32),
            vm(sine.shape, f32),
            vm((length_total, width), bf),
            vm((length_total, width), bf),
            vm((length_total, shapes[0][1]), bf),
            vm((DK, DV), f32),
            vm((length_total, heads * DV), bf),
            vm((length_total, gate.shape[1]), bf),
            vm((rows, width), bf),
            vm((rows, width), bf),
            vm((rows, width), bf),
            vm((rows, width), bf),
            vm((rows, width), bf),
            vm((heads, BLOCK, BLOCK), f32),
            vm((heads, BLOCK, BLOCK), f32),
            vm((heads, BLOCK, BLOCK), f32),
            dma((count, 5, depth)),
            dma((count, 4, depth)),
            dma((12,)),
            dma((2 + 2 * chunks,)),
            dma((2 + 2 * chunks,)),
            dma((chunks,)),
        ],
        compiler_params=pltpu.CompilerParams(
            collective_id=0, has_side_effects=True, vmem_limit_bytes=67043328
        ),
    )(*args, jnp.asarray(cosine), jnp.asarray(sine))


DK = 256
DV = 512
BLOCK = 128


norm_eps = 1e-06
rope_base = 10000.0


def rms_scale(values, gain):
    widened = values.astype(jnp.float32)
    scaled = widened * lax.rsqrt(jnp.mean(widened * widened, axis=-1, keepdims=True) + norm_eps)
    return (scaled * gain).astype(jnp.bfloat16)


def rotation(length_total, half_width):
    position = jnp.arange(length_total, dtype=jnp.float32)
    inverse = 1.0 / rope_base ** jnp.linspace(0.0, 1.0, half_width, dtype=jnp.float32)
    angle = position[:, None] * inverse[None, :]
    return (jnp.cos(angle), jnp.sin(angle))


def rotate(vectors):
    length_total = vectors.shape[0]
    half_width = vectors.shape[-1] // 2
    cosine, sine = rotation(length_total, half_width)
    cosine, sine = cosine[:, None, :], sine[:, None, :]
    first = vectors[..., :half_width]
    second = vectors[..., half_width:]
    return jnp.concatenate(
        [first * cosine - second * sine, second * cosine + first * sine], axis=-1
    )


def decay_tables(head_ids, block):
    log_gamma = jnp.log1p(-(2.0 ** (-5.0 - 2.0 * head_ids.astype(jnp.float32))))
    offset = jnp.arange(block, dtype=jnp.float32)
    distance = offset[:, None] - offset[None, :]
    inside = jnp.where(
        distance >= 0, jnp.exp(log_gamma[:, None, None] * jnp.maximum(distance, 0.0)), 0.0
    )
    query_decay = jnp.exp(log_gamma[:, None] * (offset + 1.0))
    key_decay = jnp.exp(log_gamma[:, None] * (block - 1.0 - offset))
    block_decay = jnp.exp(log_gamma * block)
    return (inside, query_decay, key_decay, block_decay)


def retain(queries, keys, values, head_ids, block):
    length_total, heads, key_width = queries.shape
    value_width = values.shape[-1]
    count = length_total // block
    inside, query_decay, key_decay, block_decay = decay_tables(head_ids, block)

    def blocks(tensor):
        return tensor.reshape(count, block, heads, tensor.shape[-1]).transpose(0, 2, 1, 3)

    def advance(memory, inputs):
        query_tile_rows, key_tile_rows, value_block = inputs
        attention_scores = jnp.einsum(
            "zvf,zjf->zvj", query_tile_rows, key_tile_rows, preferred_element_type=jnp.float32
        )
        weights = (attention_scores * inside).astype(jnp.bfloat16)
        within = jnp.einsum(
            "hlm,hmv->hlv", weights, value_block, preferred_element_type=jnp.float32
        )
        carried = (
            jnp.einsum(
                "hld,hdv->hlv",
                query_tile_rows,
                memory.astype(jnp.bfloat16),
                preferred_element_type=jnp.float32,
            )
            * query_decay[:, :, None]
        )
        weighted_keys = (key_tile_rows.astype(jnp.float32) * key_decay[:, :, None]).astype(
            jnp.bfloat16
        )
        memory = memory * block_decay[:, None, None] + jnp.einsum(
            "hld,hlv->hdv", weighted_keys, value_block, preferred_element_type=jnp.float32
        )
        return (memory, within + carried)

    start_state = jnp.zeros((heads, key_width, value_width), jnp.float32)
    _, outputs = lax.scan(advance, start_state, (blocks(queries), blocks(keys), blocks(values)))
    return outputs.transpose(0, 2, 1, 3).reshape(length_total, heads, value_width)


def head_scale(retained, gain):
    scaled = retained * lax.rsqrt(jnp.mean(retained * retained, axis=-1, keepdims=True) + norm_eps)
    return (scaled.reshape(retained.shape[0], -1) * gain).astype(jnp.bfloat16)


def swap(rows):
    return lax.ppermute(rows, "tp", [(0, 1), (1, 0)])


def join_rows(rows):
    if lax.axis_size("tp") != 2:
        return lax.all_gather(rows, "tp", axis=0, tiled=True)
    first = lax.axis_index("tp") == 0
    got = swap(rows)
    return jnp.concatenate([jnp.where(first, rows, got), jnp.where(first, got, rows)], axis=0)


def share_sum(part):
    if lax.axis_size("tp") != 2:
        summed = lax.psum_scatter(part, "tp", scatter_dimension=0, tiled=True)
        return summed.astype(jnp.float32)
    count = part.shape[0] // 2
    me = lax.axis_index("tp")
    mine = lax.dynamic_slice_in_dim(part, me * count, count, axis=0)
    theirs = lax.dynamic_slice_in_dim(part, (1 - me) * count, count, axis=0)
    return mine.astype(jnp.float32) + swap(theirs).astype(jnp.float32)


def shards(
    resid,
    mix_gain,
    query_weight,
    key_weight,
    value_weight,
    head_gain,
    out_weight,
    mlp_gain,
    gate_weight,
    up_weight,
    down_weight,
):
    token_rows = resid.shape[0]
    length_total = token_rows * lax.axis_size("tp")
    key_cols = query_weight.shape[1]
    heads_here = key_cols // DK
    shapes = [
        (query_weight.shape[0], query_weight.shape[1] + key_weight.shape[1] + value_weight.shape[1]),
        out_weight.shape,
        (gate_weight.shape[0], gate_weight.shape[1] + up_weight.shape[1]),
        down_weight.shape,
    ]
    if fits(shapes, token_rows, heads_here):
        args = [
            resid, mix_gain, query_weight, key_weight, value_weight, head_gain,
            out_weight, mlp_gain, gate_weight, up_weight, down_weight,
        ]
        return layer(args, shapes, heads_here)
    normed = rms_scale(resid, mix_gain)
    mixer_shard = jnp.concatenate([query_weight, key_weight, value_weight], axis=1)
    mlp_shard = jnp.concatenate([gate_weight, up_weight], axis=1)
    normed_full = join_rows(normed)
    head_ids = lax.axis_index("tp") * heads_here + jnp.arange(heads_here, dtype=jnp.int32)
    pieces = [mixer_shard, out_weight, mlp_shard, down_weight]
    mixer_full, out_full, mlp_full, down_full = (
        lax.all_gather(s, "fs", axis=a, tiled=True) for s, a in zip(pieces, [0, 1, 0, 1])
    )
    projected = jnp.dot(
        normed_full, mixer_full, preferred_element_type=jnp.float32
    ).astype(jnp.bfloat16)
    both_keys = projected[:, : 2 * key_cols].astype(jnp.float32)
    both_keys = both_keys.reshape(length_total, 2, heads_here, DK)
    values = projected[:, 2 * key_cols :].reshape(length_total, heads_here, DV)
    query_rot = rotate(both_keys[:, 0]).astype(jnp.bfloat16)
    key_rot = (rotate(both_keys[:, 1]) * DK ** (-0.5)).astype(jnp.bfloat16)
    retained = retain(query_rot, key_rot, values, head_ids, BLOCK)
    head_out = head_scale(retained, head_gain)
    part = jnp.dot(head_out, out_full, preferred_element_type=jnp.float32).astype(jnp.bfloat16)
    mixer_sum = share_sum(part)
    middle = (resid.astype(jnp.float32) + mixer_sum).astype(jnp.bfloat16)
    normed_mlp = rms_scale(middle, mlp_gain)
    local_units = gate_weight.shape[1]
    both = jnp.dot(
        join_rows(normed_mlp),
        mlp_full,
        preferred_element_type=jnp.float32,
    )
    hidden_units = (jax.nn.silu(both[:, :local_units]) * both[:, local_units:]).astype(jnp.bfloat16)
    mlp_sum = share_sum(
        jnp.dot(hidden_units, down_full, preferred_element_type=jnp.float32).astype(jnp.bfloat16)
    )
    return (middle.astype(jnp.float32) + mlp_sum).astype(jnp.bfloat16)


def solution(mesh):
    placed = (
        P(("rep", "fs", "tp"), None),
        P(),
        P("fs", "tp"),
        P("fs", "tp"),
        P("fs", "tp"),
        P("tp"),
        P("tp", "fs"),
        P(),
        P("fs", "tp"),
        P("fs", "tp"),
        P("tp", "fs"),
    )
    return jax.shard_map(
        shards, mesh=mesh, in_specs=placed, out_specs=P(("rep", "fs", "tp"), None), check_vma=False
    )
```

```python
import functools
import math

import jax
import jax.numpy as jnp
import numpy as np
from jax import lax
from jax.experimental import pallas as pl
from jax.experimental.pallas import tpu as pltpu
from jax.sharding import PartitionSpec as P

UNITS = 8
MESH = pl.DeviceIdType.MESH


class Stream:
    def __init__(self, w, first, count, along_z, along_y):
        self.w, self.first, self.count = w, first, count
        self.along_z, self.along_y = along_z, along_y


class Exchange:
    def __init__(self, depth, streams, shapes, axes, fulls, send_sem, recv_sem):
        self.depth, self.streams = depth, streams
        self.shapes, self.axes, self.fulls = shapes, axes, fulls
        self.send_sem, self.recv_sem = send_sem, recv_sem
        self.x = lax.axis_index("rep")
        fs = lax.axis_index("fs")
        self.z = fs // 2
        self.y = lax.rem(fs, 2)

    def barrier(self):
        sem = pltpu.get_barrier_semaphore()
        z, y, x = self.z, self.y, self.x
        core = lax.axis_index("tp")
        pl.semaphore_signal(sem, inc=1, device_id={"tp": 1 - core}, device_id_type=MESH)
        pl.semaphore_signal(sem, inc=1, device_id={"rep": 1 - x}, device_id_type=MESH)
        pl.semaphore_signal(sem, inc=1, device_id={"fs": z * 2 + 1 - y}, device_id_type=MESH)

        @pl.when(z > 0)
        def _():
            pl.semaphore_signal(sem, inc=1, device_id={"fs": (z - 1) * 2 + y}, device_id_type=MESH)

        @pl.when(z < self.depth - 1)
        def _():
            pl.semaphore_signal(sem, inc=1, device_id={"fs": (z + 1) * 2 + y}, device_id_type=MESH)

        low = jnp.minimum(z, 1)
        high = jnp.minimum(self.depth - 1 - z, 1)
        pl.semaphore_wait(sem, 3 + low + high)

    def slot(self, w, block, start, count):
        rows, cols = self.shapes[w]
        if self.axes[w] == 0:
            first = pl.multiple_of(block * rows + start, 16)
            return self.fulls[w].at[pl.ds(first, count), :]
        return self.fulls[w].at[
            pl.ds(pl.multiple_of(start, 16), count), pl.ds(pl.multiple_of(block * cols, 128), cols)
        ]

    def copy(self, s, kind, origin, incoming=False):
        stream = self.streams[s]
        x, y, z = self.x, self.y, self.z
        a, b = stream.along_z, stream.along_y
        unit = stream.count // UNITS
        xs = 1 - x if incoming and kind in ("x1", "x2") else x
        start, count = {
            "up": ((UNITS - a) * x, a),
            "down": ((UNITS - a) * x, a),
            "y": ((UNITS - b) * x, b),
            "x1": (a * xs, UNITS - a),
            "x2": (b * xs, UNITS - b),
        }[kind]
        start, count = stream.first + start * unit, count * unit
        far = kind == "x2" or (incoming and kind == "y")
        block = origin * 2 + (1 - y if far else y)
        target = {
            "up": {"fs": (z + 1) * 2 + y},
            "down": {"fs": (z - 1) * 2 + y},
            "y": {"fs": z * 2 + 1 - y},
            "x1": {"rep": 1 - x},
            "x2": {"rep": 1 - x},
        }[kind]
        place = self.slot(stream.w, block, start, count)
        sends = ("up", "down", "y", "x1", "x2").index(kind)
        receives = (0, 0, 1, 2, 3)[sends]
        return pltpu.make_async_remote_copy(
            src_ref=place,
            dst_ref=place,
            send_sem=self.send_sem.at[s, sends, origin],
            recv_sem=self.recv_sem.at[s, receives, origin],
            device_id=target,
            device_id_type=MESH,
        )

    def each(self, t, body):
        if t == 0:
            body("own", self.z)
            return

        @pl.when(self.z - t >= 0)
        def _():
            body("up", self.z - t)

        @pl.when(self.z + t < self.depth)
        def _():
            body("down", self.z + t)

    def onward(self, s, way, origin, act):
        if way in ("own", "up"):

            @pl.when(self.z < self.depth - 1)
            def _():
                act(self.copy(s, "up", origin))

        if way in ("own", "down"):

            @pl.when(self.z > 0)
            def _():
                act(self.copy(s, "down", origin))

    def step(self, s, t):
        if t < self.depth:

            def arrive(way, origin):
                if way != "own":
                    self.copy(s, way, origin, incoming=True).wait_recv()
                self.onward(s, way, origin, lambda c: c.start())
                self.copy(s, "y", origin).start()
                if way != "own":
                    self.copy(s, "x1", origin).start()

            self.each(t, arrive)
        if 1 <= t <= self.depth:

            def cross(way, origin):
                self.copy(s, "y", origin, incoming=True).wait_recv()
                self.copy(s, "x2", origin).start()

            self.each(t - 1, cross)
        if t == self.depth + 1:
            for back in range(self.depth):

                def last(way, origin):
                    if way != "own":
                        self.copy(s, "x1", origin, incoming=True).wait_recv()
                    self.copy(s, "x2", origin, incoming=True).wait_recv()

                self.each(back, last)

    def drain(self, s):
        for back in range(self.depth):

            def sent(way, origin):
                self.onward(s, way, origin, lambda c: c.wait_send())
                self.copy(s, "y", origin).wait_send()
                if way != "own":
                    self.copy(s, "x1", origin).wait_send()
                self.copy(s, "x2", origin).wait_send()

            self.each(back, sent)


class Halves:
    def __init__(self, depth, gate_up, down, far_send, far_recv, send_sem, recv_sem, sizes):
        self.depth, self.gate_up, self.down = depth, gate_up, down
        self.far_send, self.far_recv = far_send, far_recv
        self.send_sem, self.recv_sem = send_sem, recv_sem
        self.in_rows, self.out_cols = sizes
        self.x = lax.axis_index("rep")
        fs = lax.axis_index("fs")
        self.z = fs // 2
        self.y = lax.rem(fs, 2)

    def near(self, rank):
        orders = []
        for z in range(self.depth):
            orders.append(sorted(range(self.depth), key=lambda other: (abs(other - z), other)))
        code = sum(orders[z][rank] * self.depth**z for z in range(self.depth))
        place = 0
        for z in range(self.depth):
            digit = code // self.depth**z % self.depth
            place = place + digit * jnp.where(self.z == z, 1, 0)
        return place

    def block(self, s, origin):
        return origin * 2 + (self.y if s % 2 == 0 else 1 - self.y)

    def place(self, s, origin, side):
        block = self.block(s, origin)
        if s < 2:
            half = self.in_rows // 2
            start = pl.multiple_of(block * self.in_rows + side * half, 16)
            return self.gate_up.at[pl.ds(start, half), :]
        half = self.down.shape[0] // 2
        return self.down.at[
            pl.ds(pl.multiple_of(side * half, 16), half),
            pl.ds(pl.multiple_of(block * self.out_cols, 128), self.out_cols),
        ]

    def cross(self, part, incoming=False):
        mine = self.z * 2 + self.y
        block = self.z * 2 + 1 - self.y if incoming else mine
        if part < 4:
            count = self.in_rows // 4
            source = self.other_gate_up.at[pl.ds(part * count, count), :]
            start = pl.multiple_of(block * self.in_rows + part * count, 16)
            place = self.gate_up.at[pl.ds(start, count), :]
        else:
            source = self.other_down
            place = self.down.at[
                :, pl.ds(pl.multiple_of(block * self.out_cols, 128), self.out_cols)
            ]
        return pltpu.make_async_remote_copy(
            src_ref=source,
            dst_ref=place,
            send_sem=self.far_send.at[part],
            recv_sem=self.far_recv.at[part],
            device_id={"fs": self.z * 2 + 1 - self.y},
            device_id_type=MESH,
        )

    def copy(self, s, kind, origin, incoming=False):
        x, y, z = self.x, self.y, self.z
        side = 1 - x if incoming and kind == "x" else x
        target = {
            "up": {"fs": (z + 1) * 2 + y},
            "down": {"fs": (z - 1) * 2 + y},
            "x": {"rep": 1 - x},
        }[kind]
        place = self.place(s, origin, side)
        sends = ("up", "down", "x").index(kind)
        receives = (0, 0, 1)[sends]
        return pltpu.make_async_remote_copy(
            src_ref=place,
            dst_ref=place,
            send_sem=self.send_sem.at[s, sends, origin],
            recv_sem=self.recv_sem.at[s, receives, origin],
            device_id=target,
            device_id_type=MESH,
        )

    each = Exchange.each
    onward = Exchange.onward

    def step(self, s, t):
        def arrive(way, origin):
            if way != "own":
                self.copy(s, way, origin, incoming=True).wait_recv()
            self.onward(s, way, origin, lambda c: c.start())
            if way != "own":
                self.copy(s, "x", origin).start()

        self.each(t, arrive)

    def joined(self, s):
        for rank in range(1, self.depth):
            self.copy(s, "x", self.near(rank), incoming=True).wait_recv()

    def drain(self, s):
        for back in range(self.depth):

            def sent(way, origin):
                self.onward(s, way, origin, lambda c: c.wait_send())
                if way != "own":
                    self.copy(s, "x", origin).wait_send()

            self.each(back, sent)


class Near:
    def __init__(self, axis, send_sem, recv_sem):
        self.send_sem, self.recv_sem = send_sem, recv_sem
        if axis == "tp":
            self.target = {"tp": 1 - lax.axis_index("tp")}
        else:
            fs = lax.axis_index("fs")
            self.target = {"fs": fs // 2 * 2 + 1 - lax.rem(fs, 2)}

    def copy(self, index, source, place):
        return pltpu.make_async_remote_copy(
            src_ref=source,
            dst_ref=place,
            send_sem=self.send_sem.at[index],
            recv_sem=self.recv_sem.at[index],
            device_id=self.target,
            device_id_type=MESH,
        )


def rotated(v, cosine, sine):
    half = v.shape[-1] // 2
    first, second = v[:, :half], v[:, half:]
    return jnp.concatenate(
        [first * cosine - second * sine, second * cosine + first * sine], axis=-1
    )


def column_dot(left, right, out, width=256):
    @pl.loop(0, out.shape[1] // width)
    def _(c):
        cols = pl.ds(pl.multiple_of(c * width, width), width)
        out[:, cols] = jnp.dot(
            left[...], right[:, cols], preferred_element_type=jnp.float32
        ).astype(out.dtype)


def scaled_rows(values, gain):
    scale = lax.rsqrt(jnp.mean(values * values, axis=-1, keepdims=True) + norm_eps)
    return (values * scale * gain).astype(jnp.bfloat16)


def decay_rates(ids):
    return [math.log1p(-(2.0 ** (-5.0 - 2.0 * i))) for i in ids]


def make_tables(heads, inside, query_decay, key_decay):
    core = lax.axis_index("tp")
    block = inside.shape[-1]
    rates = decay_rates(range(2 * heads))
    row = lax.broadcasted_iota(jnp.int32, (block, block), 0).astype(jnp.float32)
    col = lax.broadcasted_iota(jnp.int32, (block, block), 1).astype(jnp.float32)
    distance = row - col
    for h in range(heads):
        rate = jnp.where(core == 0, rates[h], rates[heads + h])
        inside[h] = jnp.where(
            distance >= 0, jnp.exp(rate * jnp.maximum(distance, 0.0)), 0.0
        )
        query_decay[h] = jnp.exp(rate * (row + 1.0))
        key_decay[h] = jnp.exp(rate * (block - 1.0 - row))


def weigh_blocks(heads, tables, pairs, weights, decayed):
    cos_ref, sin_ref, inside, _, key_decay = tables
    block = inside.shape[-1]

    @pl.loop(0, pairs.shape[0] // block)
    def _(b):
        rows = pl.ds(pl.multiple_of(b * block, block), block)
        cosine, sine = cos_ref[rows, :], sin_ref[rows, :]
        for h in range(heads):
            q_cols = pl.ds(h * DK, DK)
            k_cols = pl.ds((heads + h) * DK, DK)
            q = rotated(pairs[rows, q_cols].astype(jnp.float32), cosine, sine)
            q = q.astype(jnp.bfloat16)
            k = rotated(pairs[rows, k_cols].astype(jnp.float32), cosine, sine) * DK ** (-0.5)
            k = k.astype(jnp.bfloat16)
            scores = lax.dot_general(
                q, k, (((1,), (1,)), ((), ())), preferred_element_type=jnp.float32
            )
            pairs[rows, q_cols] = q
            weights[rows, pl.ds(h * block, block)] = (scores * inside[h]).astype(jnp.bfloat16)
            decayed[rows, q_cols] = (
                k.astype(jnp.float32) * key_decay[h][:, 0:1]
            ).astype(jnp.bfloat16)


def retain_blocks(heads, first, last, tables, gain, held, memory, head_out):
    pairs, weights, decayed, values = held
    inside, query_decay = tables[2], tables[3]
    core = lax.axis_index("tp")
    block = inside.shape[-1]
    rates = decay_rates(range(2 * heads))
    if first == 0:
        memory[...] = jnp.zeros_like(memory)

    @pl.loop(first, last)
    def _(b):
        rows = pl.ds(pl.multiple_of(b * block, block), block)
        for h in range(heads):
            block_decay = jnp.where(
                core == 0, math.exp(rates[h] * block), math.exp(rates[heads + h] * block)
            )
            v_cols = pl.ds(h * DV, DV)
            v = values[rows, v_cols]
            state = memory[h]
            kept = jnp.dot(
                weights[rows, pl.ds(h * block, block)], v, preferred_element_type=jnp.float32
            ) + query_decay[h][:, 0:1] * jnp.dot(
                pairs[rows, pl.ds(h * DK, DK)],
                state.astype(jnp.bfloat16),
                preferred_element_type=jnp.float32,
            )
            memory[h] = state * block_decay + lax.dot_general(
                decayed[rows, pl.ds(h * DK, DK)],
                v,
                (((0,), (0,)), ((), ())),
                preferred_element_type=jnp.float32,
            )
            scale = lax.rsqrt(jnp.mean(kept * kept, axis=-1, keepdims=True) + norm_eps)
            head_out[rows, v_cols] = (kept * scale * gain[:, v_cols]).astype(jnp.bfloat16)


ROWS = 64
WIDE = 512
TILE = 128
SHARED = 3


def layer_kernel(depth, streams, shapes, heads, *refs):
    args, refs = refs[:13], refs[13:]
    resid, mix_gain, query, key, value, head_gain, out_w, mlp_gain, gate, up, down, cos, sin = args
    out, refs = refs[0], refs[1:]
    fulls, refs = refs[:3], refs[3:]
    pair_full, value_full, out_full = fulls
    gate_up, other_gate_up, down_full, other_down, refs = *refs[:4], refs[4:]
    x, gain_mix, gain_head, gain_mlp, cos_v, sin_v, middle_gate, middle_up, refs = (
        *refs[:8],
        refs[8:],
    )
    normed, both, pairs, values, weights, decayed, memory, head_out, hidden, refs = (
        *refs[:9],
        refs[9:],
    )
    part, sent, got, far_part, far_sent, far_got, far_sum, far_in, middle, refs = (
        *refs[:9],
        refs[9:],
    )
    inside, query_decay, key_decay, refs = *refs[:3], refs[3:]
    send_sem, recv_sem, half_send, half_recv, cross_send, cross_recv, refs = *refs[:6], refs[6:]
    load_sem, peer_send, peer_recv, beside_send, beside_recv, out_sem = refs

    ex = Exchange(depth, streams, shapes, (0, 0, 1), fulls, send_sem, recv_sem)
    sizes = (gate.shape[0], down.shape[1])
    hv = Halves(
        depth, gate_up, down_full, cross_send, cross_recv, half_send, half_recv, sizes
    )
    hv.other_gate_up, hv.other_down = other_gate_up, other_down
    peer = Near("tp", peer_send, peer_recv)
    beside = Near("fs", beside_send, beside_recv)
    core = lax.axis_index("tp")
    fs = lax.axis_index("fs")
    y = lax.rem(fs, 2)
    rows, width = x.shape
    qc, kc = query.shape[1], key.shape[1]
    units = gate.shape[1]
    whole = units // 2 // TILE
    aligned = whole * TILE
    step = aligned + TILE
    blocks = width // sizes[1]

    own_rows = ex.slot(0, fs, 0, shapes[0][0])
    first_row = pl.multiple_of(fs * shapes[0][0], 16)
    own_pair = pl.ds(first_row, shapes[0][0])
    own_cols = pl.ds(pl.multiple_of(fs * sizes[1], 128), sizes[1])

    def down_pieces(side, place):
        rest = units // 2 - aligned
        return [
            (down.at[pl.ds(pl.multiple_of(side * step, 16), aligned), :], place(0, aligned)),
            (
                down.at[pl.ds(pl.multiple_of(aligned + side * rest, 16), rest), :],
                place(aligned, rest),
            ),
        ]

    moves = [
        (query, pair_full.at[own_pair, pl.ds(0, qc)]),
        (key, pair_full.at[own_pair, pl.ds(qc, kc)]),
        (value, ex.slot(1, fs, 0, shapes[1][0])),
        (resid, x),
        (mix_gain, gain_mix),
        (out_w, ex.slot(2, fs, 0, shapes[2][0])),
        (gate.at[:, pl.ds(aligned, TILE)], middle_gate),
        (up.at[:, pl.ds(aligned, TILE)], middle_up),
        *down_pieces(y, lambda start, count: down_full.at[pl.ds(start, count), own_cols]),
        *down_pieces(1 - y, lambda start, count: other_down.at[pl.ds(start, count), :]),
        (cos, cos_v),
        (sin, sin_v),
        (head_gain, gain_head),
        (mlp_gain, gain_mlp),
    ]
    loads = [
        pltpu.make_async_copy(source, place, load_sem.at[i])
        for i, (source, place) in enumerate(moves)
    ]
    for load in loads[:8]:
        load.start()
    own_gate_up = gate_up.at[own_pair, :]
    gathers = []
    for side, target, index in ((y, own_gate_up, 0), (1 - y, other_gate_up, 1)):
        sem = load_sem.at[len(moves) + index]

        @pl.loop(0, whole)
        def _(j):
            cols = pl.ds(pl.multiple_of(side * step + j * TILE, TILE), TILE)
            for i, source in enumerate((gate, up)):
                place = pl.ds(pl.multiple_of(j * 2 * TILE, TILE) + i * TILE, TILE)
                pltpu.make_async_copy(source.at[:, cols], target.at[:, place], sem).start()

        bulk = target.at[:, pl.ds(0, 2 * aligned)]
        gathers.append(pltpu.make_async_copy(bulk, bulk, sem))
    for load in loads[8:]:
        load.start()

    ex.barrier()

    def chip_rows(side, of):
        return pl.ds(pl.multiple_of((side * 2 + of) * rows, 16), rows)

    own = pl.ds(pl.multiple_of(core * rows, 16), rows)
    other = pl.ds(pl.multiple_of((1 - core) * rows, 16), rows)
    join_mix = peer.copy(0, normed.at[own, :], normed.at[own, :])

    def norm_mix():
        loads[3].wait()
        loads[4].wait()

        @pl.loop(0, rows // ROWS)
        def _(r):
            here = pl.ds(pl.multiple_of(r * ROWS, ROWS), ROWS)
            there = pl.ds(pl.multiple_of(core * rows + r * ROWS, ROWS), ROWS)
            normed[there, :] = scaled_rows(x[here, :].astype(jnp.float32), gain_mix[...])

        join_mix.start()
        loads[6].wait()
        loads[7].wait()
        half = TILE // 2
        low_gate = middle_gate[...].astype(jnp.float32)
        low_up = middle_up[...].astype(jnp.float32)
        first = jnp.concatenate([low_gate[:, :half], low_up[:, :half]], axis=1)
        second = jnp.concatenate([low_gate[:, half:], low_up[:, half:]], axis=1)
        end = pl.ds(2 * aligned, TILE)
        mine = jnp.where(y == 0, first, second)
        theirs = jnp.where(y == 0, second, first)
        gate_up[own_pair, end] = mine.astype(jnp.bfloat16)
        other_gate_up[:, end] = theirs.astype(jnp.bfloat16)
        make_tables(heads, inside, query_decay, key_decay)
        for load in loads[12:]:
            load.wait()
        for load in gathers:
            load.wait()

    def cross(parts):
        for part_index in parts:
            if part_index == 4:
                for load in loads[8:12]:
                    load.wait()
            hv.cross(part_index).start()

    tables = (cos_v, sin_v, inside, query_decay, key_decay)
    held = (pairs, weights, decayed, values)

    def project_pairs():
        join_mix.wait()
        column_dot(normed, pair_full, pairs)
        weigh_blocks(heads, tables, pairs, weights, decayed)

    def project_values():
        column_dot(normed, value_full, values)

    def retain_some(first, last):
        retain_blocks(heads, first, last, tables, gain_head, held, memory, head_out)

    chunks = width // WIDE

    def share(index, c):
        cols = pl.ds(c * WIDE, WIDE)
        return peer.copy(index + c, sent.at[:, cols], got.at[:, cols])

    def product(left, theirs, mine, right, index):
        for rows_of, place in ((theirs, sent), (mine, part)):
            for c in range(chunks):

                @pl.loop(0, WIDE // 256)
                def _(i):
                    cols = pl.ds(pl.multiple_of(c * WIDE + i * 256, 256), 256)
                    place[:, cols] = jnp.dot(
                        left[rows_of, :], right[:, cols], preferred_element_type=jnp.float32
                    ).astype(jnp.bfloat16)

                if place is sent:
                    share(index, c).start()

    def shared_rows(side, of, i):
        count = rows // SHARED
        start = pl.multiple_of((side * 2 + of) * rows + i * count, 16)
        return both.at[pl.ds(start, count), :]

    def join_own(i, of):
        place = shared_rows(y, of, i)
        return peer.copy(1 + i, place, place)

    def join_far(i, of):
        place = shared_rows(1 - y, of, i)
        return peer.copy(1 + SHARED + i, place, place)

    def join_beside(i, side):
        place = shared_rows(side, core, i)
        return beside.copy(i, place, place)

    base = 1 + 2 * SHARED

    def norm_mlp():
        for c in range(chunks):
            share(base, c).wait()
        count = rows // SHARED
        for i in range(SHARED):

            @pl.loop(0, count // ROWS)
            def _(r):
                at = i * count + r * ROWS
                here = pl.ds(pl.multiple_of(at, ROWS), ROWS)
                there = pl.ds(pl.multiple_of((y * 2 + core) * rows + at, ROWS), ROWS)
                total = part[here, :].astype(jnp.float32) + got[here, :].astype(jnp.float32)
                mid = (x[here, :].astype(jnp.float32) + total).astype(jnp.bfloat16)
                middle[here, :] = mid
                both[there, :] = scaled_rows(mid.astype(jnp.float32), gain_mlp[...])

            join_beside(i, y).start()
            join_own(i, core).start()

    def pass_on(i):
        join_beside(i, 1 - y).wait_recv()
        join_far(i, core).start()

    def expand(side):
        tokens = pl.ds(pl.multiple_of(side * 2 * rows, 16), 2 * rows)

        @pl.loop(0, whole)
        def _(j):
            cols = pl.ds(pl.multiple_of(j * 2 * TILE, 2 * TILE), 2 * TILE)
            two = jnp.dot(both[tokens, :], gate_up[:, cols], preferred_element_type=jnp.float32)
            place = pl.ds(pl.multiple_of(j * TILE, TILE), TILE)
            hidden[tokens, place] = (jax.nn.silu(two[:, :TILE]) * two[:, TILE:]).astype(
                jnp.bfloat16
            )

        two = jnp.dot(
            both[tokens, :],
            gate_up[:, pl.ds(2 * aligned, TILE)],
            preferred_element_type=jnp.float32,
        )
        half = TILE // 2
        hidden[tokens, pl.ds(aligned, half)] = (
            jax.nn.silu(two[:, :half]) * two[:, half:]
        ).astype(jnp.bfloat16)

    def expand_far():
        for s in (0, 1):
            hv.joined(s)
        for i in range(SHARED):
            join_far(i, 1 - core).wait_recv()
        expand(1 - y)

    def block_cols(block):
        return pl.ds(pl.multiple_of(block * sizes[1], 128), sizes[1])

    over = base + chunks

    def swap_far(block):
        cols = block_cols(block)
        return peer.copy(over + block, far_sent.at[:, cols], far_got.at[:, cols])

    def give(block):
        cols = block_cols(block)
        return beside.copy(SHARED + block, far_sum.at[:, cols], far_in.at[:, cols])

    def reduce_far(block):
        cols = block_cols(block)
        far_sent[:, cols] = jnp.dot(
            hidden[chip_rows(1 - y, 1 - core), :],
            down_full[:, cols],
            preferred_element_type=jnp.float32,
        ).astype(jnp.bfloat16)
        swap_far(block).start()
        far_part[:, cols] = jnp.dot(
            hidden[chip_rows(1 - y, core), :],
            down_full[:, cols],
            preferred_element_type=jnp.float32,
        ).astype(jnp.bfloat16)

    def give_far(block):
        cols = block_cols(block)
        swap_far(block).wait_recv()
        total = far_part[:, cols].astype(jnp.float32) + far_got[:, cols].astype(jnp.float32)
        far_sum[:, cols] = total.astype(jnp.bfloat16)
        give(block).start()

    def reduce_rank(rank):
        origin = hv.near(rank)
        for s in (2, 3):
            if rank == 0 and s == 3:
                pass
            if rank > 0:
                hv.copy(s, "x", origin, incoming=True).wait_recv()
            reduce_far(hv.block(s, origin))
        for s in (2, 3):
            give_far(hv.block(s, origin))

    last = over + blocks

    def own_part():
        for i in range(SHARED):
            join_own(i, 1 - core).wait_recv()
        expand(y)
        product(hidden, chip_rows(y, 1 - core), chip_rows(y, core), down_full, last)

    def finish():
        writes = []
        for c in range(chunks):
            share(last, c).wait()
        for rank in range(depth):
            origin = hv.near(rank)
            for s in (3, 2):
                block = hv.block(s, origin)
                cols = block_cols(block)
                give(block).wait_recv()
                total = part[:, cols].astype(jnp.float32) + got[:, cols].astype(jnp.float32)
                total = total + far_in[:, cols].astype(jnp.float32)
                middle[:, cols] = (middle[:, cols].astype(jnp.float32) + total).astype(
                    jnp.bfloat16
                )
                write = pltpu.make_async_copy(
                    middle.at[:, cols], out.at[:, cols], out_sem.at[block]
                )
                write.start()
                writes.append(write)
        for write in writes:
            write.wait()

    plan = {}

    def at(tick, *jobs):
        plan.setdefault(tick, []).extend(jobs)

    stages = len(streams) // 2
    turn = 2 * (depth - 1)
    at(0, norm_mix)
    for i in range(4):
        at(2 + i, functools.partial(cross, (i,)))
    at(8, functools.partial(cross, (4,)))
    at(turn + 4, project_pairs)
    at(turn + 5, project_values)
    length = pairs.shape[0] // inside.shape[-1]
    at(turn + 6, functools.partial(retain_some, 0, length // 2))
    at(turn + 7, functools.partial(retain_some, length // 2, length))
    at(
        2 * turn + 5,
        lambda: product(head_out, other, own, out_full, base),
        norm_mlp,
    )
    mlp_at = stages * turn
    at(2 * turn + 7, functools.partial(pass_on, 0))
    at(2 * turn + 8, functools.partial(pass_on, 1))
    at(mlp_at + turn + 3, functools.partial(pass_on, 2), expand_far)
    at(mlp_at + turn + 3, functools.partial(reduce_rank, 0))
    at(mlp_at + turn + 4, functools.partial(reduce_rank, 1))
    at(mlp_at + turn + 5, functools.partial(reduce_rank, 2))
    at(mlp_at + turn + 7, functools.partial(reduce_rank, 3), own_part, finish)
    begin = {0: loads[:2], 1: loads[2:3], 2: loads[5:6]}
    for tick in range(mlp_at + 2 * turn + 2):
        for s in range(len(streams)):
            t, odd = divmod(tick - turn * (s // 2), 2)
            if odd == s % 2 and 0 <= t <= depth + 1:
                if t == 0:
                    for load in begin.get(s, ()):
                        load.wait()
                ex.step(s, t)
        for s in range(4):
            t, odd = divmod(tick - mlp_at - turn * (s // 2), 2)
            if odd == s % 2 and 0 <= t < depth:
                if t == 0 and s % 2 == 1:
                    for part_index in range(4) if s == 1 else (4,):
                        hv.cross(part_index, incoming=True).wait_recv()
                hv.step(s, t)
        for job in plan.get(tick, ()):
            job()
    for s in range(len(streams)):
        ex.drain(s)
    for s in range(4):
        hv.drain(s)
    for part_index in range(5):
        hv.cross(part_index).wait_send()
    for i in range(SHARED):
        join_own(i, core).wait_send()
        join_far(i, core).wait_send()
        join_beside(i, y).wait_send()
    for block in range(blocks):
        swap_far(block).wait_send()
        give(block).wait_send()


def plan_streams(shapes):
    streams = []
    for w, (rows, _) in enumerate(shapes[:2]):
        streams.append(Stream(w, 0, rows, 6 + w, 4))
    half = shapes[2][0] // 2
    streams.append(Stream(2, 0, half, 6, 4))
    streams.append(Stream(2, half, half, 7, 4))
    return streams


def rotation_tables(length_total, half_width):
    position = np.arange(length_total, dtype=np.float32)
    inverse = (1.0 / rope_base ** np.linspace(0.0, 1.0, half_width)).astype(np.float32)
    angle = (position[:, None] * inverse[None, :]).astype(np.float64)
    return np.cos(angle).astype(np.float32), np.sin(angle).astype(np.float32)


def fits(shapes, rows, width, heads, units):
    whole = all(r % (2 * UNITS * 16) == 0 and c % 128 == 0 for r, c in shapes)
    axes = lax.axis_size("rep") == 2 and lax.axis_size("fs") == 8 and lax.axis_size("tp") == 2
    cut = units % (2 * TILE) == TILE and width % WIDE == 0 and width == 8 * shapes[2][1]
    return whole and axes and cut and rows % (SHARED * ROWS) == 0 and heads == 2


def layer(args, shapes, heads):
    resid, gate, down = args[0], args[8], args[10]
    size = lax.axis_size("fs")
    depth = size // 2
    rows, width = resid.shape
    length_total = 2 * rows
    units = gate.shape[1]
    streams = plan_streams(shapes)
    count = len(streams)
    fulls = []
    for (r, c), axis in zip(shapes, (0, 0, 1)):
        fulls.append((r * size, c) if axis == 0 else (r, c * size))
    cosine, sine = rotation_tables(length_total, DK // 2)
    far = pl.BlockSpec(memory_space=pl.ANY)
    bf, f32 = jnp.bfloat16, jnp.float32
    vm = pltpu.VMEM
    dma = pltpu.SemaphoreType.DMA
    chunks = width // WIDE
    peers = 1 + 2 * SHARED + 2 * chunks + size
    args = [a[None, :] if a.ndim == 1 else a for a in args]
    return pl.pallas_call(
        functools.partial(layer_kernel, depth, streams, shapes, heads),
        out_shape=jax.ShapeDtypeStruct((rows, width), bf),
        in_specs=[far] * 13,
        out_specs=far,
        scratch_shapes=[vm(s, bf) for s in fulls]
        + [
            vm((gate.shape[0] * size, units), bf),
            vm((gate.shape[0], units), bf),
            vm((units // 2, width), bf),
            vm((units // 2, down.shape[1]), bf),
            vm((rows, width), bf),
            vm(args[1].shape, f32),
            vm(args[5].shape, f32),
            vm(args[7].shape, f32),
            vm(cosine.shape, f32),
            vm(sine.shape, f32),
            vm((gate.shape[0], TILE), bf),
            vm((gate.shape[0], TILE), bf),
            vm((length_total, width), bf),
            vm((2 * length_total, width), bf),
            vm((length_total, shapes[0][1]), bf),
            vm((length_total, shapes[1][1]), bf),
            vm((length_total, heads * BLOCK), bf),
            vm((length_total, heads * DK), bf),
            vm((heads, DK, DV), f32),
            vm((length_total, heads * DV), bf),
            vm((2 * length_total, units // 2), bf),
        ]
        + [vm((rows, width), bf)] * 9
        + [vm((heads, BLOCK, BLOCK), f32)] * 3
        + [
            dma((count, 5, depth)),
            dma((count, 4, depth)),
            dma((4, 3, depth)),
            dma((4, 2, depth)),
            dma((5,)),
            dma((5,)),
            dma((18,)),
            dma((peers,)),
            dma((peers,)),
            dma((SHARED + size,)),
            dma((SHARED + size,)),
            dma((size,)),
        ],
        compiler_params=pltpu.CompilerParams(
            collective_id=0, has_side_effects=True, vmem_limit_bytes=67043328
        ),
    )(*args, jnp.asarray(cosine), jnp.asarray(sine))


DK = 256
DV = 512
BLOCK = 128


norm_eps = 1e-06
rope_base = 10000.0


def rms_scale(values, gain):
    widened = values.astype(jnp.float32)
    scaled = widened * lax.rsqrt(jnp.mean(widened * widened, axis=-1, keepdims=True) + norm_eps)
    return (scaled * gain).astype(jnp.bfloat16)


def rotation(length_total, half_width):
    position = jnp.arange(length_total, dtype=jnp.float32)
    inverse = 1.0 / rope_base ** jnp.linspace(0.0, 1.0, half_width, dtype=jnp.float32)
    angle = position[:, None] * inverse[None, :]
    return (jnp.cos(angle), jnp.sin(angle))


def rotate(vectors):
    length_total = vectors.shape[0]
    half_width = vectors.shape[-1] // 2
    cosine, sine = rotation(length_total, half_width)
    cosine, sine = cosine[:, None, :], sine[:, None, :]
    first = vectors[..., :half_width]
    second = vectors[..., half_width:]
    return jnp.concatenate(
        [first * cosine - second * sine, second * cosine + first * sine], axis=-1
    )


def decay_tables(head_ids, block):
    log_gamma = jnp.log1p(-(2.0 ** (-5.0 - 2.0 * head_ids.astype(jnp.float32))))
    offset = jnp.arange(block, dtype=jnp.float32)
    distance = offset[:, None] - offset[None, :]
    inside = jnp.where(
        distance >= 0, jnp.exp(log_gamma[:, None, None] * jnp.maximum(distance, 0.0)), 0.0
    )
    query_decay = jnp.exp(log_gamma[:, None] * (offset + 1.0))
    key_decay = jnp.exp(log_gamma[:, None] * (block - 1.0 - offset))
    block_decay = jnp.exp(log_gamma * block)
    return (inside, query_decay, key_decay, block_decay)


def retain(queries, keys, values, head_ids, block):
    length_total, heads, key_width = queries.shape
    value_width = values.shape[-1]
    count = length_total // block
    inside, query_decay, key_decay, block_decay = decay_tables(head_ids, block)

    def blocks(tensor):
        return tensor.reshape(count, block, heads, tensor.shape[-1]).transpose(0, 2, 1, 3)

    def advance(memory, inputs):
        query_tile_rows, key_tile_rows, value_block = inputs
        attention_scores = jnp.einsum(
            "zvf,zjf->zvj", query_tile_rows, key_tile_rows, preferred_element_type=jnp.float32
        )
        weights = (attention_scores * inside).astype(jnp.bfloat16)
        within = jnp.einsum(
            "hlm,hmv->hlv", weights, value_block, preferred_element_type=jnp.float32
        )
        carried = (
            jnp.einsum(
                "hld,hdv->hlv",
                query_tile_rows,
                memory.astype(jnp.bfloat16),
                preferred_element_type=jnp.float32,
            )
            * query_decay[:, :, None]
        )
        weighted_keys = (key_tile_rows.astype(jnp.float32) * key_decay[:, :, None]).astype(
            jnp.bfloat16
        )
        memory = memory * block_decay[:, None, None] + jnp.einsum(
            "hld,hlv->hdv", weighted_keys, value_block, preferred_element_type=jnp.float32
        )
        return (memory, within + carried)

    start_state = jnp.zeros((heads, key_width, value_width), jnp.float32)
    _, outputs = lax.scan(advance, start_state, (blocks(queries), blocks(keys), blocks(values)))
    return outputs.transpose(0, 2, 1, 3).reshape(length_total, heads, value_width)


def head_scale(retained, gain):
    scaled = retained * lax.rsqrt(jnp.mean(retained * retained, axis=-1, keepdims=True) + norm_eps)
    return (scaled.reshape(retained.shape[0], -1) * gain).astype(jnp.bfloat16)


def swap(rows):
    return lax.ppermute(rows, "tp", [(0, 1), (1, 0)])


def join_rows(rows):
    if lax.axis_size("tp") != 2:
        return lax.all_gather(rows, "tp", axis=0, tiled=True)
    first = lax.axis_index("tp") == 0
    got = swap(rows)
    return jnp.concatenate([jnp.where(first, rows, got), jnp.where(first, got, rows)], axis=0)


def share_sum(part):
    if lax.axis_size("tp") != 2:
        summed = lax.psum_scatter(part, "tp", scatter_dimension=0, tiled=True)
        return summed.astype(jnp.float32)
    count = part.shape[0] // 2
    me = lax.axis_index("tp")
    mine = lax.dynamic_slice_in_dim(part, me * count, count, axis=0)
    theirs = lax.dynamic_slice_in_dim(part, (1 - me) * count, count, axis=0)
    return mine.astype(jnp.float32) + swap(theirs).astype(jnp.float32)


def shards(
    resid,
    mix_gain,
    query_weight,
    key_weight,
    value_weight,
    head_gain,
    out_weight,
    mlp_gain,
    gate_weight,
    up_weight,
    down_weight,
):
    token_rows = resid.shape[0]
    length_total = token_rows * lax.axis_size("tp")
    key_cols = query_weight.shape[1]
    heads_here = key_cols // DK
    shapes = [
        (query_weight.shape[0], query_weight.shape[1] + key_weight.shape[1]),
        value_weight.shape,
        out_weight.shape,
    ]
    if fits(shapes, token_rows, resid.shape[1], heads_here, gate_weight.shape[1]):
        args = [
            resid, mix_gain, query_weight, key_weight, value_weight, head_gain,
            out_weight, mlp_gain, gate_weight, up_weight, down_weight,
        ]
        return layer(args, shapes, heads_here)
    normed = rms_scale(resid, mix_gain)
    mixer_shard = jnp.concatenate([query_weight, key_weight, value_weight], axis=1)
    mlp_shard = jnp.concatenate([gate_weight, up_weight], axis=1)
    normed_full = join_rows(normed)
    head_ids = lax.axis_index("tp") * heads_here + jnp.arange(heads_here, dtype=jnp.int32)
    pieces = [mixer_shard, out_weight, mlp_shard, down_weight]
    mixer_full, out_full, mlp_full, down_full = (
        lax.all_gather(s, "fs", axis=a, tiled=True) for s, a in zip(pieces, [0, 1, 0, 1])
    )
    projected = jnp.dot(
        normed_full, mixer_full, preferred_element_type=jnp.float32
    ).astype(jnp.bfloat16)
    both_keys = projected[:, : 2 * key_cols].astype(jnp.float32)
    both_keys = both_keys.reshape(length_total, 2, heads_here, DK)
    values = projected[:, 2 * key_cols :].reshape(length_total, heads_here, DV)
    query_rot = rotate(both_keys[:, 0]).astype(jnp.bfloat16)
    key_rot = (rotate(both_keys[:, 1]) * DK ** (-0.5)).astype(jnp.bfloat16)
    retained = retain(query_rot, key_rot, values, head_ids, BLOCK)
    head_out = head_scale(retained, head_gain)
    part = jnp.dot(head_out, out_full, preferred_element_type=jnp.float32).astype(jnp.bfloat16)
    mixer_sum = share_sum(part)
    middle = (resid.astype(jnp.float32) + mixer_sum).astype(jnp.bfloat16)
    normed_mlp = rms_scale(middle, mlp_gain)
    local_units = gate_weight.shape[1]
    both = jnp.dot(
        join_rows(normed_mlp),
        mlp_full,
        preferred_element_type=jnp.float32,
    )
    hidden_units = (jax.nn.silu(both[:, :local_units]) * both[:, local_units:]).astype(jnp.bfloat16)
    mlp_sum = share_sum(
        jnp.dot(hidden_units, down_full, preferred_element_type=jnp.float32).astype(jnp.bfloat16)
    )
    return (middle.astype(jnp.float32) + mlp_sum).astype(jnp.bfloat16)


def solution(mesh):
    placed = (
        P(("rep", "fs", "tp"), None),
        P(),
        P("fs", "tp"),
        P("fs", "tp"),
        P("fs", "tp"),
        P("tp"),
        P("tp", "fs"),
        P(),
        P("fs", "tp"),
        P("fs", "tp"),
        P("tp", "fs"),
    )
    return jax.shard_map(
        shards, mesh=mesh, in_specs=placed, out_specs=P(("rep", "fs", "tp"), None), check_vma=False
    )
```

```python
import functools
import math

import jax
import jax.numpy as jnp
import numpy as np
from jax import lax
from jax.experimental import pallas as pl
from jax.experimental.pallas import tpu as pltpu
from jax.sharding import PartitionSpec as P

MESH = pl.DeviceIdType.MESH
ROWS = 64
TILE = 128


class Weight:
    def __init__(self, full, other, axis):
        self.full, self.other, self.axis = full, other, axis
        self.rows, self.cols = other.shape


class Gather:
    def __init__(self, depth, weights, along, cross_sems, sems):
        self.depth, self.weights, self.along = depth, weights, along
        self.cross_send, self.cross_recv = cross_sems
        self.send_sem, self.recv_sem = sems
        self.x = lax.axis_index("rep")
        fs = lax.axis_index("fs")
        self.z = fs // 2
        self.y = lax.rem(fs, 2)

    def barrier(self):
        sem = pltpu.get_barrier_semaphore()
        z, y, x = self.z, self.y, self.x
        core = lax.axis_index("tp")
        pl.semaphore_signal(sem, inc=1, device_id={"tp": 1 - core}, device_id_type=MESH)
        pl.semaphore_signal(sem, inc=1, device_id={"rep": 1 - x}, device_id_type=MESH)
        pl.semaphore_signal(sem, inc=1, device_id={"fs": z * 2 + 1 - y}, device_id_type=MESH)

        @pl.when(z > 0)
        def _():
            pl.semaphore_signal(sem, inc=1, device_id={"fs": (z - 1) * 2 + y}, device_id_type=MESH)

        @pl.when(z < self.depth - 1)
        def _():
            pl.semaphore_signal(sem, inc=1, device_id={"fs": (z + 1) * 2 + y}, device_id_type=MESH)

        low = jnp.minimum(z, 1)
        high = jnp.minimum(self.depth - 1 - z, 1)
        pl.semaphore_wait(sem, 3 + low + high)

    def near(self, rank):
        place = 0
        for z in range(self.depth):
            order = sorted(range(self.depth), key=lambda other: (abs(other - z), other))
            place = place + order[rank] * jnp.where(self.z == z, 1, 0)
        return place

    def block(self, far, origin):
        return origin * 2 + (1 - self.y if far else self.y)

    def place(self, w, block, start, count):
        weight = self.weights[w]
        if weight.axis == 0:
            first = pl.multiple_of(block * weight.rows + start, 16)
            return weight.full.at[pl.ds(first, count), :]
        cols = pl.ds(pl.multiple_of(block * weight.cols, 128), weight.cols)
        return weight.full.at[pl.ds(pl.multiple_of(start, 16), count), cols]

    def cross(self, s, incoming=False):
        w = s // 2
        count = self.along[w]
        start = pl.multiple_of((self.weights[w].rows - count) * self.x, 16)
        block = self.z * 2 + (1 - self.y if incoming else self.y)
        return pltpu.make_async_remote_copy(
            src_ref=self.weights[w].other.at[pl.ds(start, count), :],
            dst_ref=self.place(w, block, start, count),
            send_sem=self.cross_send.at[w],
            recv_sem=self.cross_recv.at[w],
            device_id={"fs": self.z * 2 + 1 - self.y},
            device_id_type=MESH,
        )

    def copy(self, s, kind, origin, incoming=False):
        w, far = s // 2, s % 2
        x, y, z = self.x, self.y, self.z
        rows, along = self.weights[w].rows, self.along[w]
        if kind == "x":
            count = rows - along
            start = along * (1 - x if incoming else x)
        else:
            count = along
            start = (rows - along) * x
        target = {
            "up": {"fs": (z + 1) * 2 + y},
            "down": {"fs": (z - 1) * 2 + y},
            "x": {"rep": 1 - x},
        }[kind]
        place = self.place(w, self.block(far, origin), start, count)
        sends = ("up", "down", "x").index(kind)
        receives = (0, 0, 1)[sends]
        return pltpu.make_async_remote_copy(
            src_ref=place,
            dst_ref=place,
            send_sem=self.send_sem.at[s, sends, origin],
            recv_sem=self.recv_sem.at[s, receives, origin],
            device_id=target,
            device_id_type=MESH,
        )

    def each(self, t, body):
        if t == 0:
            body("own", self.z)
            return

        @pl.when(self.z - t >= 0)
        def _():
            body("up", self.z - t)

        @pl.when(self.z + t < self.depth)
        def _():
            body("down", self.z + t)

    def onward(self, s, way, origin, act):
        if way in ("own", "up"):

            @pl.when(self.z < self.depth - 1)
            def _():
                act(self.copy(s, "up", origin))

        if way in ("own", "down"):

            @pl.when(self.z > 0)
            def _():
                act(self.copy(s, "down", origin))

    def arrive(self, s, t):
        def body(way, origin):
            if way != "own":
                self.copy(s, way, origin, incoming=True).wait_recv()
            elif s % 2:
                self.cross(s, incoming=True).wait_recv()
            self.onward(s, way, origin, lambda c: c.start())
            if way != "own" or s % 2:
                self.copy(s, "x", origin).start()

        self.each(t, body)

    def joined(self, s, rank):
        if rank > 0 or s % 2:
            self.copy(s, "x", self.near(rank), incoming=True).wait_recv()

    def drain(self, s):
        for back in range(self.depth):

            def sent(way, origin):
                self.onward(s, way, origin, lambda c: c.wait_send())
                if way != "own" or s % 2:
                    self.copy(s, "x", origin).wait_send()

            self.each(back, sent)
        if s % 2:
            self.cross(s).wait_send()


class Near:
    def __init__(self, axis, send_sem, recv_sem):
        self.send_sem, self.recv_sem = send_sem, recv_sem
        if axis == "tp":
            self.target = {"tp": 1 - lax.axis_index("tp")}
        else:
            fs = lax.axis_index("fs")
            self.target = {"fs": fs // 2 * 2 + 1 - lax.rem(fs, 2)}

    def copy(self, layer, index, source, place):
        return pltpu.make_async_remote_copy(
            src_ref=source,
            dst_ref=place,
            send_sem=self.send_sem.at[layer, index],
            recv_sem=self.recv_sem.at[layer, index],
            device_id=self.target,
            device_id_type=MESH,
        )


def rotated(v, cosine, sine):
    half = v.shape[-1] // 2
    first, second = v[:, :half], v[:, half:]
    return jnp.concatenate(
        [first * cosine - second * sine, second * cosine + first * sine], axis=-1
    )


def scaled_rows(values, gain):
    scale = lax.rsqrt(jnp.mean(values * values, axis=-1, keepdims=True) + norm_eps)
    return (values * scale * gain).astype(jnp.bfloat16)


def head_rate(scale, power=False):
    core = lax.axis_index("tp")
    y = lax.rem(lax.axis_index("fs"), 2)
    rates = [scale * math.log1p(-(2.0 ** (-5.0 - 2.0 * i))) for i in range(4)]
    if power:
        rates = [math.exp(r) for r in rates]
    return jnp.where(
        core == 0,
        jnp.where(y == 0, rates[0], rates[1]),
        jnp.where(y == 0, rates[2], rates[3]),
    )


def make_tables(inside, query_decay, key_decay):
    block = inside.shape[-1]
    row = lax.broadcasted_iota(jnp.int32, (block, block), 0).astype(jnp.float32)
    col = lax.broadcasted_iota(jnp.int32, (block, block), 1).astype(jnp.float32)
    distance = row - col
    rate = head_rate(1.0)
    inside[...] = jnp.where(distance >= 0, jnp.exp(rate * jnp.maximum(distance, 0.0)), 0.0)
    query_decay[...] = jnp.exp(rate * (row + 1.0))
    key_decay[...] = jnp.exp(rate * (block - 1.0 - row))


def weigh_blocks(start, length, tables, pairs, weights, decayed):
    cos_ref, sin_ref, inside, _, key_decay = tables
    block = inside.shape[-1]

    @pl.loop(0, length // block)
    def _(b):
        here = pl.ds(pl.multiple_of(b * block, block), block)
        rows = pl.ds(pl.multiple_of(start + b * block, block), block)
        cosine, sine = cos_ref[here, :], sin_ref[here, :]
        q = rotated(pairs[rows, pl.ds(0, DK)].astype(jnp.float32), cosine, sine)
        q = q.astype(jnp.bfloat16)
        k = rotated(pairs[rows, pl.ds(DK, DK)].astype(jnp.float32), cosine, sine) * DK ** (-0.5)
        k = k.astype(jnp.bfloat16)
        scores = lax.dot_general(
            q, k, (((1,), (1,)), ((), ())), preferred_element_type=jnp.float32
        )
        pairs[rows, pl.ds(0, DK)] = q
        weights[rows, :] = (scores * inside[...]).astype(jnp.bfloat16)
        decayed[rows, :] = (k.astype(jnp.float32) * key_decay[:, 0:1]).astype(jnp.bfloat16)


def retain_blocks(start, length, tables, gain, held, memory, head_out):
    pairs, weights, decayed, values = held
    inside, query_decay = tables[2], tables[3]
    block = inside.shape[-1]
    block_decay = head_rate(float(block), power=True)
    memory[...] = jnp.zeros_like(memory)

    @pl.loop(0, length // block)
    def _(b):
        rows = pl.ds(pl.multiple_of(start + b * block, block), block)
        v = values[rows, :]
        state = memory[...]
        kept = jnp.dot(weights[rows, :], v, preferred_element_type=jnp.float32) + query_decay[
            :, 0:1
        ] * jnp.dot(
            pairs[rows, pl.ds(0, DK)],
            state.astype(jnp.bfloat16),
            preferred_element_type=jnp.float32,
        )
        memory[...] = state * block_decay + lax.dot_general(
            decayed[rows, :], v, (((0,), (0,)), ((), ())), preferred_element_type=jnp.float32
        )
        scale = lax.rsqrt(jnp.mean(kept * kept, axis=-1, keepdims=True) + norm_eps)
        head_out[rows, :] = (kept * scale * gain[...]).astype(jnp.bfloat16)


def layer_kernel(depth, splits, along, *refs):
    args, refs = refs[:13], refs[13:]
    resid, mix_gain, query, key, value, head_gain, out_w, mlp_gain, gate, up, down, cos, sin = args
    out, refs = refs[0], refs[1:]
    fulls, others, refs = refs[:5], refs[5:10], refs[10:]
    pair_full, value_full, out_full, gate_up, down_full = fulls
    pair_other, value_other, out_other, gate_up_other, down_other = others
    x, gain_mix, gain_head, gain_mlp, cos_v, sin_v, middle_gate, middle_up, refs = (
        *refs[:8],
        refs[8:],
    )
    normed, both, pairs, values, weights, decayed, memory, head_out, hidden, refs = (
        *refs[:9],
        refs[9:],
    )
    part, sent, got, far_part, far_sent, far_got, far_sum, far_in, middle, refs = (
        *refs[:9],
        refs[9:],
    )
    inside, query_decay, key_decay, refs = *refs[:3], refs[3:]
    send_sem, recv_sem, cross_send, cross_recv, refs = *refs[:4], refs[4:]
    load_sem, peer_send, peer_recv, beside_send, beside_recv, out_sem = refs

    axes = (0, 0, 1, 0, 1)
    ga = Gather(
        depth,
        [Weight(*given) for given in zip(fulls, others, axes)],
        along,
        (cross_send, cross_recv),
        (send_sem, recv_sem),
    )
    peer = Near("tp", peer_send, peer_recv)
    beside = Near("fs", beside_send, beside_recv)
    core = lax.axis_index("tp")
    fs = lax.axis_index("fs")
    y = lax.rem(fs, 2)
    rows, width = x.shape
    units = gate.shape[1]
    whole = units // 2 // TILE
    aligned = whole * TILE
    step = aligned + TILE
    cols_of = down.shape[1]
    blocks = width // cols_of

    def own(w):
        weight = ga.weights[w]
        return ga.place(w, fs, 0, weight.rows)

    shard = query.shape[0]
    own_rows = pl.ds(pl.multiple_of(fs * shard, 16), shard)
    own_cols = pl.ds(pl.multiple_of(fs * cols_of, 128), cols_of)

    def heads(ref, side, size):
        return ref.at[:, pl.ds(pl.multiple_of(side * size, 128), size)]

    def down_pieces(side, place):
        rest = units // 2 - aligned
        return [
            (down.at[pl.ds(pl.multiple_of(side * step, 16), aligned), :], place(0, aligned)),
            (
                down.at[pl.ds(pl.multiple_of(aligned + side * rest, 16), rest), :],
                place(aligned, rest),
            ),
        ]

    moves = [
        (heads(query, y, DK), pair_full.at[own_rows, pl.ds(0, DK)]),
        (heads(key, y, DK), pair_full.at[own_rows, pl.ds(DK, DK)]),
        (heads(query, 1 - y, DK), pair_other.at[:, pl.ds(0, DK)]),
        (heads(key, 1 - y, DK), pair_other.at[:, pl.ds(DK, DK)]),
        (heads(value, y, DV), own(1)),
        (heads(value, 1 - y, DV), value_other),
        (resid, x),
        (mix_gain, gain_mix),
        (out_w.at[pl.ds(pl.multiple_of(y * DV, 16), DV), :], own(2)),
        (out_w.at[pl.ds(pl.multiple_of((1 - y) * DV, 16), DV), :], out_other),
        (gate.at[:, pl.ds(aligned, TILE)], middle_gate),
        (up.at[:, pl.ds(aligned, TILE)], middle_up),
        *down_pieces(y, lambda start, count: down_full.at[pl.ds(start, count), own_cols]),
        *down_pieces(1 - y, lambda start, count: down_other.at[pl.ds(start, count), :]),
        (cos, cos_v),
        (sin, sin_v),
        (heads(head_gain, y, DV), gain_head),
        (mlp_gain, gain_mlp),
    ]
    loads = [
        pltpu.make_async_copy(source, place, load_sem.at[i])
        for i, (source, place) in enumerate(moves)
    ]
    for load in loads[:10]:
        load.start()
    gathers = []
    for side, target, index in ((y, own(3), 0), (1 - y, gate_up_other, 1)):
        sem = load_sem.at[len(moves) + index]

        @pl.loop(0, whole)
        def _(j):
            cols = pl.ds(pl.multiple_of(side * step + j * TILE, TILE), TILE)
            for i, source in enumerate((gate, up)):
                place = pl.ds(pl.multiple_of(j * 2 * TILE, TILE) + i * TILE, TILE)
                pltpu.make_async_copy(source.at[:, cols], target.at[:, place], sem).start()

        bulk = target.at[:, pl.ds(0, 2 * aligned)]
        gathers.append(pltpu.make_async_copy(bulk, bulk, sem))
    for load in loads[10:]:
        load.start()

    ga.barrier()

    waited = set()

    def once(name, waits):
        if name not in waited:
            waited.add(name)
            for wait in waits:
                wait()

    def loaded(*indices):
        for i in indices:
            once(("load", i), [loads[i].wait])

    def side_of(far):
        return 1 - y if far else y

    def chip_rows(far, of):
        return pl.ds(pl.multiple_of((side_of(far) * 2 + of) * rows, 16), rows)

    def chip_start(far):
        return pl.multiple_of(side_of(far) * 2 * rows, 16)

    def tokens(far):
        return pl.ds(chip_start(far), 2 * rows)

    streams = (normed, both)
    starts = [sum(splits[:i]) for i in range(len(splits))]

    def rows_at(layer, far, of, i):
        start = pl.multiple_of((side_of(far) * 2 + of) * rows + starts[i], 16)
        return streams[layer].at[pl.ds(start, splits[i]), :]

    def join_own(layer, i, of):
        place = rows_at(layer, 0, of, i)
        return peer.copy(layer, i, place, place)

    def join_far(layer, i, of):
        place = rows_at(layer, 1, of, i)
        return peer.copy(layer, len(splits) + i, place, place)

    def join_beside(layer, i, far):
        place = rows_at(layer, far, core, i)
        return beside.copy(layer, i, place, place)

    def block_cols(block):
        return pl.ds(pl.multiple_of(block * cols_of, 128), cols_of)

    def share(layer, block):
        cols = block_cols(block)
        return peer.copy(layer, 2 * len(splits) + block, sent.at[:, cols], got.at[:, cols])

    def swap_far(layer, block):
        cols = block_cols(block)
        index = 2 * len(splits) + blocks + block
        return peer.copy(layer, index, far_sent.at[:, cols], far_got.at[:, cols])

    def give(layer, block):
        cols = block_cols(block)
        return beside.copy(layer, len(splits) + block, far_sum.at[:, cols], far_in.at[:, cols])

    def spread(layer, i):
        join_beside(layer, i, 0).start()
        join_own(layer, i, core).start()

    def norm_mix():
        loaded(6, 7)
        for i, count in enumerate(splits):

            @pl.loop(0, count // ROWS)
            def _(r):
                at = starts[i] + r * ROWS
                here = pl.ds(pl.multiple_of(at, ROWS), ROWS)
                there = pl.ds(pl.multiple_of((y * 2 + core) * rows + at, ROWS), ROWS)
                normed[there, :] = scaled_rows(x[here, :].astype(jnp.float32), gain_mix[...])

            spread(0, i)
        loaded(10, 11)
        half = TILE // 2
        low_gate = middle_gate[...].astype(jnp.float32)
        low_up = middle_up[...].astype(jnp.float32)
        first = jnp.concatenate([low_gate[:, :half], low_up[:, :half]], axis=1)
        second = jnp.concatenate([low_gate[:, half:], low_up[:, half:]], axis=1)
        end = pl.ds(2 * aligned, TILE)
        mine = jnp.where(y == 0, first, second)
        theirs = jnp.where(y == 0, second, first)
        gate_up[own_rows, end] = mine.astype(jnp.bfloat16)
        gate_up_other[:, end] = theirs.astype(jnp.bfloat16)
        make_tables(inside, query_decay, key_decay)

    ready = {
        0: (0, 1), 1: (2, 3), 2: (4,), 3: (5,), 4: (8,), 5: (9,), 6: (), 7: (), 8: (12, 13),
        9: (14, 15),
    }

    def prepared(s):
        loaded(*ready[s])
        if s in (6, 7):
            once(("gather", s), [gathers[s - 6].wait])

    def h(s, t):
        if t == 0 and s % 2 == 0:
            prepared(s)
        ga.arrive(s, t)

    def cross(s):
        prepared(s)
        ga.cross(s).start()

    def pass_on(layer, i):
        join_beside(layer, i, 1).wait_recv()
        join_far(layer, i, core).start()

    def gathered(w):
        once(
            ("weight", w),
            [
                functools.partial(ga.joined, 2 * w + far, rank)
                for rank in range(depth)
                for far in (0, 1)
            ],
        )

    def arrived(layer, far, i):
        join = join_far if far else join_own
        once(("rows", layer, far, i), [lambda: join(layer, i, 1 - core).wait_recv()])

    def project(w, far, place):
        gathered(w)
        for i in range(len(splits)):
            arrived(0, far, i)
        here = tokens(far)
        full = fulls[w]

        @pl.loop(0, full.shape[1] // 256)
        def _(c):
            cols = pl.ds(pl.multiple_of(c * 256, 256), 256)
            place[here, cols] = jnp.dot(
                normed[here, :], full[:, cols], preferred_element_type=jnp.float32
            ).astype(jnp.bfloat16)

    tables = (cos_v, sin_v, inside, query_decay, key_decay)

    def pairs_of(far):
        project(0, far, pairs)
        loaded(16, 17)
        weigh_blocks(chip_start(far), 2 * rows, tables, pairs, weights, decayed)

    def values_of(far):
        project(1, far, values)

    def retain(far):
        loaded(18, 19)
        held = (pairs, weights, decayed, values)
        retain_blocks(chip_start(far), 2 * rows, tables, gain_head, held, memory, head_out)

    lefts, rights = (head_out, hidden), (out_full, down_full)

    def product(layer, far, of, block, place):
        cols = block_cols(block)
        place[:, cols] = jnp.dot(
            lefts[layer][chip_rows(far, of), :],
            rights[layer][:, cols],
            preferred_element_type=jnp.float32,
        ).astype(jnp.bfloat16)

    def far_rank(layer, rank):
        origin = ga.near(rank)
        for far in (0, 1):
            ga.joined((4, 8)[layer] + far, rank)
            block = ga.block(far, origin)
            if layer == 1:
                swap_far(0, block).wait_send()
                give(0, block).wait_send()
            product(layer, 1, 1 - core, block, far_sent)
            swap_far(layer, block).start()
            product(layer, 1, core, block, far_part)
        for far in (0, 1):
            block = ga.block(far, origin)
            cols = block_cols(block)
            swap_far(layer, block).wait_recv()
            total = far_part[:, cols].astype(jnp.float32) + far_got[:, cols].astype(jnp.float32)
            far_sum[:, cols] = total.astype(jnp.bfloat16)
            give(layer, block).start()

    def own_rank(layer, rank):
        for far in (0, 1):
            block = ga.block(far, ga.near(rank))
            product(layer, 0, 1 - core, block, sent)
            share(layer, block).start()
            product(layer, 0, core, block, part)

    def norm_mlp():
        for block in range(blocks):
            share(0, block).wait()
        for block in range(blocks):
            give(0, block).wait_recv()
        for i, count in enumerate(splits):

            @pl.loop(0, count // ROWS)
            def _(r):
                at = starts[i] + r * ROWS
                here = pl.ds(pl.multiple_of(at, ROWS), ROWS)
                there = pl.ds(pl.multiple_of((y * 2 + core) * rows + at, ROWS), ROWS)
                total = part[here, :].astype(jnp.float32) + got[here, :].astype(jnp.float32)
                total = total + far_in[here, :].astype(jnp.float32)
                mid = (x[here, :].astype(jnp.float32) + total).astype(jnp.bfloat16)
                middle[here, :] = mid
                both[there, :] = scaled_rows(mid.astype(jnp.float32), gain_mlp[...])

            spread(1, i)

    def activate(ranges):
        @pl.loop(0, whole)
        def _(j):
            cols = pl.ds(pl.multiple_of(j * 2 * TILE, 2 * TILE), 2 * TILE)
            place = pl.ds(pl.multiple_of(j * TILE, TILE), TILE)
            for here in ranges:
                two = jnp.dot(both[here, :], gate_up[:, cols], preferred_element_type=jnp.float32)
                hidden[here, place] = (jax.nn.silu(two[:, :TILE]) * two[:, TILE:]).astype(
                    jnp.bfloat16
                )

        half = TILE // 2
        for here in ranges:
            two = jnp.dot(
                both[here, :],
                gate_up[:, pl.ds(2 * aligned, TILE)],
                preferred_element_type=jnp.float32,
            )
            hidden[here, pl.ds(aligned, half)] = (
                jax.nn.silu(two[:, :half]) * two[:, half:]
            ).astype(jnp.bfloat16)

    def expand(far, i=None):
        gathered(3)
        if far:
            arrived(1, 1, i)
            activate(
                [
                    pl.ds(
                        pl.multiple_of((side_of(1) * 2 + of) * rows + starts[i], 16), splits[i]
                    )
                    for of in (0, 1)
                ]
            )
        else:
            for part_index in range(len(splits)):
                arrived(1, 0, part_index)
            activate([tokens(0)])

    def finish():
        for block in range(blocks):
            share(1, block).wait()
        writes = []
        for rank in range(depth):
            origin = ga.near(rank)
            for far in (1, 0):
                block = ga.block(far, origin)
                cols = block_cols(block)
                give(1, block).wait_recv()
                total = part[:, cols].astype(jnp.float32) + got[:, cols].astype(jnp.float32)
                total = total + far_in[:, cols].astype(jnp.float32)
                middle[:, cols] = (middle[:, cols].astype(jnp.float32) + total).astype(
                    jnp.bfloat16
                )
                write = pltpu.make_async_copy(
                    middle.at[:, cols], out.at[:, cols], out_sem.at[block]
                )
                write.start()
                writes.append(write)
        for write in writes:
            write.wait()

    order = [
        (h, 2, 0), (h, 0, 0), (cross, 3), (cross, 1), (norm_mix,), (cross, 5), (h, 3, 0),
        (h, 2, 1), (h, 1, 0), (h, 2, 2), (h, 1, 1), (h, 2, 3), (h, 3, 1), (cross, 9), (h, 0, 1),
        (h, 3, 2), (h, 0, 2), (pass_on, 0, 0), (h, 4, 0), (h, 3, 3), (h, 1, 2), (h, 1, 3),
        (h, 0, 3), (h, 6, 0), (pass_on, 0, 1), (values_of, 0), (h, 5, 0), (cross, 7),
        (values_of, 1), (h, 4, 1), (pairs_of, 1), (retain, 1), (h, 5, 1), (far_rank, 0, 0),
        (h, 4, 2), (pairs_of, 0), (h, 5, 2), (far_rank, 0, 1), (h, 6, 1), (h, 4, 3), (retain, 0),
        (h, 5, 3), (far_rank, 0, 2), (h, 7, 0), (far_rank, 0, 3), (h, 6, 2), (own_rank, 0, 3),
        (h, 7, 1), (own_rank, 0, 2), (own_rank, 0, 1), (own_rank, 0, 0), (h, 9, 0), (norm_mlp,),
        (h, 6, 3), (h, 7, 2), (h, 7, 3), (h, 9, 1), (h, 8, 0), (pass_on, 1, 0), (h, 8, 1),
        (h, 9, 2), (expand, 1, 0), (pass_on, 1, 1), (h, 8, 2), (h, 9, 3), (expand, 1, 1),
        (far_rank, 1, 1), (far_rank, 1, 0), (expand, 0), (h, 8, 3), (own_rank, 1, 1),
        (far_rank, 1, 2), (own_rank, 1, 0), (own_rank, 1, 2), (far_rank, 1, 3), (own_rank, 1, 3),
        (finish,),
    ]
    for job, *given in order:
        job(*given)
    for s in range(2 * len(fulls)):
        ga.drain(s)
    for layer in (0, 1):
        for i in range(len(splits)):
            join_own(layer, i, core).wait_send()
            join_far(layer, i, core).wait_send()
            join_beside(layer, i, 0).wait_send()
    for block in range(blocks):
        swap_far(1, block).wait_send()
        give(1, block).wait_send()


def rotation_tables(length_total, half_width):
    position = np.arange(length_total, dtype=np.float32)
    inverse = (1.0 / rope_base ** np.linspace(0.0, 1.0, half_width)).astype(np.float32)
    angle = (position[:, None] * inverse[None, :]).astype(np.float64)
    return np.cos(angle).astype(np.float32), np.sin(angle).astype(np.float32)


def fits(rows, width, key_cols, value_cols, units, shard, out_cols):
    axes = lax.axis_size("rep") == 2 and lax.axis_size("fs") == 8 and lax.axis_size("tp") == 2
    cut = units % (2 * TILE) == TILE and (units // 2) % 32 == 0
    whole = width == 8 * out_cols and width == 8 * shard and shard % 256 == 0
    heads = key_cols == 2 * DK and value_cols == 2 * DV
    return axes and cut and whole and heads and rows % 192 == 0


def layer(args):
    resid, query, gate, down = args[0], args[2], args[8], args[10]
    size = lax.axis_size("fs")
    depth = size // 2
    rows, width = resid.shape
    tokens = 4 * rows
    units = gate.shape[1]
    shard, out_cols = query.shape[0], down.shape[1]
    others = [(shard, 2 * DK), (shard, DV), (DV, out_cols), (shard, units), (units // 2, out_cols)]
    fulls = []
    for (r, c), axis in zip(others, (0, 0, 1, 0, 1)):
        fulls.append((r * size, c) if axis == 0 else (r, c * size))
    along = [shard // 2, shard // 2, DV // 2, shard // 16 * 9 // 16 * 16, units // 2 // 2]
    splits = (2 * rows // 3, rows // 3)
    cosine, sine = rotation_tables(2 * rows, DK // 2)
    far = pl.BlockSpec(memory_space=pl.ANY)
    bf, f32 = jnp.bfloat16, jnp.float32
    vm = pltpu.VMEM
    dma = pltpu.SemaphoreType.DMA
    slices = 2 * len(fulls)
    peers = 2 * len(splits) + 2 * size
    args = [a[None, :] if a.ndim == 1 else a for a in args]
    return pl.pallas_call(
        functools.partial(layer_kernel, depth, splits, along),
        out_shape=jax.ShapeDtypeStruct((rows, width), bf),
        in_specs=[far] * 13,
        out_specs=far,
        scratch_shapes=[vm(s, bf) for s in fulls]
        + [vm(s, bf) for s in others]
        + [
            vm((rows, width), bf),
            vm(args[1].shape, f32),
            vm((1, DV), f32),
            vm(args[7].shape, f32),
            vm(cosine.shape, f32),
            vm(sine.shape, f32),
            vm((shard, TILE), bf),
            vm((shard, TILE), bf),
            vm((tokens, width), bf),
            vm((tokens, width), bf),
            vm((tokens, 2 * DK), bf),
            vm((tokens, DV), bf),
            vm((tokens, BLOCK), bf),
            vm((tokens, DK), bf),
            vm((DK, DV), f32),
            vm((tokens, DV), bf),
            vm((tokens, units // 2), bf),
        ]
        + [vm((rows, width), bf)] * 9
        + [vm((BLOCK, BLOCK), f32)] * 3
        + [
            dma((slices, 3, depth)),
            dma((slices, 2, depth)),
            dma((len(fulls),)),
            dma((len(fulls),)),
            dma((22,)),
            dma((2, peers)),
            dma((2, peers)),
            dma((2, len(splits) + size)),
            dma((2, len(splits) + size)),
            dma((size,)),
        ],
        compiler_params=pltpu.CompilerParams(
            collective_id=0, has_side_effects=True, vmem_limit_bytes=67043328
        ),
    )(*args, jnp.asarray(cosine), jnp.asarray(sine))


DK = 256
DV = 512
BLOCK = 128


norm_eps = 1e-06
rope_base = 10000.0


def rms_scale(values, gain):
    widened = values.astype(jnp.float32)
    scaled = widened * lax.rsqrt(jnp.mean(widened * widened, axis=-1, keepdims=True) + norm_eps)
    return (scaled * gain).astype(jnp.bfloat16)


def rotation(length_total, half_width):
    position = jnp.arange(length_total, dtype=jnp.float32)
    inverse = 1.0 / rope_base ** jnp.linspace(0.0, 1.0, half_width, dtype=jnp.float32)
    angle = position[:, None] * inverse[None, :]
    return (jnp.cos(angle), jnp.sin(angle))


def rotate(vectors):
    length_total = vectors.shape[0]
    half_width = vectors.shape[-1] // 2
    cosine, sine = rotation(length_total, half_width)
    cosine, sine = cosine[:, None, :], sine[:, None, :]
    first = vectors[..., :half_width]
    second = vectors[..., half_width:]
    return jnp.concatenate(
        [first * cosine - second * sine, second * cosine + first * sine], axis=-1
    )


def decay_tables(head_ids, block):
    log_gamma = jnp.log1p(-(2.0 ** (-5.0 - 2.0 * head_ids.astype(jnp.float32))))
    offset = jnp.arange(block, dtype=jnp.float32)
    distance = offset[:, None] - offset[None, :]
    inside = jnp.where(
        distance >= 0, jnp.exp(log_gamma[:, None, None] * jnp.maximum(distance, 0.0)), 0.0
    )
    query_decay = jnp.exp(log_gamma[:, None] * (offset + 1.0))
    key_decay = jnp.exp(log_gamma[:, None] * (block - 1.0 - offset))
    block_decay = jnp.exp(log_gamma * block)
    return (inside, query_decay, key_decay, block_decay)


def retain(queries, keys, values, head_ids, block):
    length_total, heads, key_width = queries.shape
    value_width = values.shape[-1]
    count = length_total // block
    inside, query_decay, key_decay, block_decay = decay_tables(head_ids, block)

    def blocks(tensor):
        return tensor.reshape(count, block, heads, tensor.shape[-1]).transpose(0, 2, 1, 3)

    def advance(memory, inputs):
        query_tile_rows, key_tile_rows, value_block = inputs
        attention_scores = jnp.einsum(
            "zvf,zjf->zvj", query_tile_rows, key_tile_rows, preferred_element_type=jnp.float32
        )
        weights = (attention_scores * inside).astype(jnp.bfloat16)
        within = jnp.einsum(
            "hlm,hmv->hlv", weights, value_block, preferred_element_type=jnp.float32
        )
        carried = (
            jnp.einsum(
                "hld,hdv->hlv",
                query_tile_rows,
                memory.astype(jnp.bfloat16),
                preferred_element_type=jnp.float32,
            )
            * query_decay[:, :, None]
        )
        weighted_keys = (key_tile_rows.astype(jnp.float32) * key_decay[:, :, None]).astype(
            jnp.bfloat16
        )
        memory = memory * block_decay[:, None, None] + jnp.einsum(
            "hld,hlv->hdv", weighted_keys, value_block, preferred_element_type=jnp.float32
        )
        return (memory, within + carried)

    start_state = jnp.zeros((heads, key_width, value_width), jnp.float32)
    _, outputs = lax.scan(advance, start_state, (blocks(queries), blocks(keys), blocks(values)))
    return outputs.transpose(0, 2, 1, 3).reshape(length_total, heads, value_width)


def head_scale(retained, gain):
    scaled = retained * lax.rsqrt(jnp.mean(retained * retained, axis=-1, keepdims=True) + norm_eps)
    return (scaled.reshape(retained.shape[0], -1) * gain).astype(jnp.bfloat16)


def swap(rows):
    return lax.ppermute(rows, "tp", [(0, 1), (1, 0)])


def join_rows(rows):
    if lax.axis_size("tp") != 2:
        return lax.all_gather(rows, "tp", axis=0, tiled=True)
    first = lax.axis_index("tp") == 0
    got = swap(rows)
    return jnp.concatenate([jnp.where(first, rows, got), jnp.where(first, got, rows)], axis=0)


def share_sum(part):
    if lax.axis_size("tp") != 2:
        summed = lax.psum_scatter(part, "tp", scatter_dimension=0, tiled=True)
        return summed.astype(jnp.float32)
    count = part.shape[0] // 2
    me = lax.axis_index("tp")
    mine = lax.dynamic_slice_in_dim(part, me * count, count, axis=0)
    theirs = lax.dynamic_slice_in_dim(part, (1 - me) * count, count, axis=0)
    return mine.astype(jnp.float32) + swap(theirs).astype(jnp.float32)


def shards(
    resid,
    mix_gain,
    query_weight,
    key_weight,
    value_weight,
    head_gain,
    out_weight,
    mlp_gain,
    gate_weight,
    up_weight,
    down_weight,
):
    token_rows = resid.shape[0]
    length_total = token_rows * lax.axis_size("tp")
    key_cols = query_weight.shape[1]
    heads_here = key_cols // DK
    sizes = (
        token_rows, resid.shape[1], key_cols, value_weight.shape[1], gate_weight.shape[1],
        query_weight.shape[0], down_weight.shape[1],
    )
    if fits(*sizes):
        args = [
            resid, mix_gain, query_weight, key_weight, value_weight, head_gain,
            out_weight, mlp_gain, gate_weight, up_weight, down_weight,
        ]
        return layer(args)
    normed = rms_scale(resid, mix_gain)
    mixer_shard = jnp.concatenate([query_weight, key_weight, value_weight], axis=1)
    mlp_shard = jnp.concatenate([gate_weight, up_weight], axis=1)
    normed_full = join_rows(normed)
    head_ids = lax.axis_index("tp") * heads_here + jnp.arange(heads_here, dtype=jnp.int32)
    pieces = [mixer_shard, out_weight, mlp_shard, down_weight]
    mixer_full, out_full, mlp_full, down_full = (
        lax.all_gather(s, "fs", axis=a, tiled=True) for s, a in zip(pieces, [0, 1, 0, 1])
    )
    projected = jnp.dot(
        normed_full, mixer_full, preferred_element_type=jnp.float32
    ).astype(jnp.bfloat16)
    both_keys = projected[:, : 2 * key_cols].astype(jnp.float32)
    both_keys = both_keys.reshape(length_total, 2, heads_here, DK)
    values = projected[:, 2 * key_cols :].reshape(length_total, heads_here, DV)
    query_rot = rotate(both_keys[:, 0]).astype(jnp.bfloat16)
    key_rot = (rotate(both_keys[:, 1]) * DK ** (-0.5)).astype(jnp.bfloat16)
    retained = retain(query_rot, key_rot, values, head_ids, BLOCK)
    head_out = head_scale(retained, head_gain)
    part = jnp.dot(head_out, out_full, preferred_element_type=jnp.float32).astype(jnp.bfloat16)
    mixer_sum = share_sum(part)
    middle = (resid.astype(jnp.float32) + mixer_sum).astype(jnp.bfloat16)
    normed_mlp = rms_scale(middle, mlp_gain)
    local_units = gate_weight.shape[1]
    both = jnp.dot(
        join_rows(normed_mlp),
        mlp_full,
        preferred_element_type=jnp.float32,
    )
    hidden_units = (jax.nn.silu(both[:, :local_units]) * both[:, local_units:]).astype(jnp.bfloat16)
    mlp_sum = share_sum(
        jnp.dot(hidden_units, down_full, preferred_element_type=jnp.float32).astype(jnp.bfloat16)
    )
    return (middle.astype(jnp.float32) + mlp_sum).astype(jnp.bfloat16)


def solution(mesh):
    placed = (
        P(("rep", "fs", "tp"), None),
        P(),
        P("fs", "tp"),
        P("fs", "tp"),
        P("fs", "tp"),
        P("tp"),
        P("tp", "fs"),
        P(),
        P("fs", "tp"),
        P("fs", "tp"),
        P("tp", "fs"),
    )
    return jax.shard_map(
        shards, mesh=mesh, in_specs=placed, out_specs=P(("rep", "fs", "tp"), None), check_vma=False
    )
```

```python
import functools
import math

import jax
import jax.numpy as jnp
import numpy as np
from jax import lax
from jax.experimental import pallas as pl
from jax.experimental.pallas import tpu as pltpu
from jax.sharding import PartitionSpec as P

MESH = pl.DeviceIdType.MESH
ROWS = 64
TILE = 128


class Weight:
    def __init__(self, full, other, axis):
        self.full, self.other, self.axis = full, other, axis
        self.rows, self.cols = other.shape


class Gather:
    def __init__(self, depth, weights, along, cross_sems, sems):
        self.depth, self.weights, self.along = depth, weights, along
        self.cross_send, self.cross_recv = cross_sems
        self.send_sem, self.recv_sem = sems
        self.x = lax.axis_index("rep")
        fs = lax.axis_index("fs")
        self.z = fs // 2
        self.y = lax.rem(fs, 2)

    def greet(self):
        sem = pltpu.get_barrier_semaphore()
        z, y, x = self.z, self.y, self.x
        core = lax.axis_index("tp")
        pl.semaphore_signal(sem, inc=1, device_id={"tp": 1 - core}, device_id_type=MESH)
        pl.semaphore_signal(sem, inc=1, device_id={"rep": 1 - x}, device_id_type=MESH)
        pl.semaphore_signal(sem, inc=1, device_id={"fs": z * 2 + 1 - y}, device_id_type=MESH)

        @pl.when(z > 0)
        def _():
            pl.semaphore_signal(sem, inc=1, device_id={"fs": (z - 1) * 2 + y}, device_id_type=MESH)

        @pl.when(z < self.depth - 1)
        def _():
            pl.semaphore_signal(sem, inc=1, device_id={"fs": (z + 1) * 2 + y}, device_id_type=MESH)

    def meet(self):
        low = jnp.minimum(self.z, 1)
        high = jnp.minimum(self.depth - 1 - self.z, 1)
        pl.semaphore_wait(pltpu.get_barrier_semaphore(), 3 + low + high)

    def near(self, rank):
        place = 0
        for z in range(self.depth):
            order = sorted(range(self.depth), key=lambda other: (abs(other - z), other))
            place = place + order[rank] * jnp.where(self.z == z, 1, 0)
        return place

    def block(self, far, origin):
        return origin * 2 + (1 - self.y if far else self.y)

    def place(self, w, block, start, count):
        weight = self.weights[w]
        if weight.axis == 0:
            first = pl.multiple_of(block * weight.rows + start, 16)
            return weight.full.at[pl.ds(first, count), :]
        cols = pl.ds(pl.multiple_of(block * weight.cols, 128), weight.cols)
        return weight.full.at[pl.ds(pl.multiple_of(start, 16), count), cols]

    def cross(self, s, incoming=False):
        w = s // 2
        count = self.along[w]
        start = pl.multiple_of((self.weights[w].rows - count) * self.x, 16)
        block = self.z * 2 + (1 - self.y if incoming else self.y)
        return pltpu.make_async_remote_copy(
            src_ref=self.weights[w].other.at[pl.ds(start, count), :],
            dst_ref=self.place(w, block, start, count),
            send_sem=self.cross_send.at[w],
            recv_sem=self.cross_recv.at[w],
            device_id={"fs": self.z * 2 + 1 - self.y},
            device_id_type=MESH,
        )

    def copy(self, s, kind, origin, incoming=False, own=False):
        w, far = s // 2, s % 2
        x, y, z = self.x, self.y, self.z
        rows, along = self.weights[w].rows, self.along[w]
        if kind == "x":
            count = rows - along
            start = along * (1 - x if incoming else x)
        else:
            count = along
            start = (rows - along) * x
        target = {
            "up": {"fs": (z + 1) * 2 + y},
            "down": {"fs": (z - 1) * 2 + y},
            "x": {"rep": 1 - x},
        }[kind]
        place = self.place(w, self.block(far, origin), start, count)
        slot = origin
        if kind == "x":
            slot = self.depth + origin
        elif kind == "down" and own:
            slot = 2 * self.depth
        return pltpu.make_async_remote_copy(
            src_ref=place,
            dst_ref=place,
            send_sem=self.send_sem.at[s, slot],
            recv_sem=self.recv_sem.at[s, origin + (self.depth if kind == "x" else 0)],
            device_id=target,
            device_id_type=MESH,
        )

    def each(self, t, body):
        if t == 0:
            body("own", self.z)
            return

        @pl.when(self.z - t >= 0)
        def _():
            body("up", self.z - t)

        @pl.when(self.z + t < self.depth)
        def _():
            body("down", self.z + t)

    def onward(self, s, way, origin, act):
        if way in ("own", "up"):

            @pl.when(self.z < self.depth - 1)
            def _():
                act(self.copy(s, "up", origin))

        if way in ("own", "down"):

            @pl.when(self.z > 0)
            def _():
                act(self.copy(s, "down", origin, own=way == "own"))

    def arrive(self, s, t):
        def body(way, origin):
            if way != "own":
                self.copy(s, way, origin, incoming=True).wait_recv()
            elif s % 2:
                self.cross(s, incoming=True).wait_recv()
            self.onward(s, way, origin, lambda c: c.start())
            if way != "own" or s % 2:
                self.copy(s, "x", origin).start()

        self.each(t, body)

    def joined(self, s, rank):
        if rank > 0 or s % 2:
            self.copy(s, "x", self.near(rank), incoming=True).wait_recv()

    def drain(self, s):
        for back in range(self.depth):

            def sent(way, origin):
                self.onward(s, way, origin, lambda c: c.wait_send())
                if way != "own" or s % 2:
                    self.copy(s, "x", origin).wait_send()

            self.each(back, sent)
        if s % 2:
            self.cross(s).wait_send()


class Near:
    def __init__(self, axis, send_sem, recv_sem):
        self.send_sem, self.recv_sem = send_sem, recv_sem
        if axis == "tp":
            self.target = {"tp": 1 - lax.axis_index("tp")}
        else:
            fs = lax.axis_index("fs")
            self.target = {"fs": fs // 2 * 2 + 1 - lax.rem(fs, 2)}

    def copy(self, index, source, place):
        return pltpu.make_async_remote_copy(
            src_ref=source,
            dst_ref=place,
            send_sem=self.send_sem.at[index],
            recv_sem=self.recv_sem.at[index],
            device_id=self.target,
            device_id_type=MESH,
        )


def rotated(v, cosine, sine):
    half = v.shape[-1] // 2
    first, second = v[:, :half], v[:, half:]
    return jnp.concatenate(
        [first * cosine - second * sine, second * cosine + first * sine], axis=-1
    )


def scaled_rows(values, gain):
    scale = lax.rsqrt(jnp.mean(values * values, axis=-1, keepdims=True) + norm_eps)
    return (values * scale * gain).astype(jnp.bfloat16)


def head_rate(scale, power=False):
    core = lax.axis_index("tp")
    y = lax.rem(lax.axis_index("fs"), 2)
    rates = [scale * math.log1p(-(2.0 ** (-5.0 - 2.0 * i))) for i in range(4)]
    if power:
        rates = [math.exp(r) for r in rates]
    return jnp.where(
        core == 0,
        jnp.where(y == 0, rates[0], rates[1]),
        jnp.where(y == 0, rates[2], rates[3]),
    )


def make_tables(inside, query_decay, key_decay):
    block = inside.shape[-1]
    row = lax.broadcasted_iota(jnp.int32, (block, block), 0).astype(jnp.float32)
    col = lax.broadcasted_iota(jnp.int32, (block, block), 1).astype(jnp.float32)
    distance = row - col
    rate = head_rate(1.0)
    inside[...] = jnp.where(distance >= 0, jnp.exp(rate * jnp.maximum(distance, 0.0)), 0.0)
    query_decay[...] = jnp.exp(rate * (row + 1.0))
    key_decay[...] = jnp.exp(rate * (block - 1.0 - row))


def weigh_blocks(start, length, tables, pairs, weights, decayed):
    cos_ref, sin_ref, inside, _, key_decay = tables
    block = inside.shape[-1]

    @pl.loop(0, length // block)
    def _(b):
        here = pl.ds(pl.multiple_of(b * block, block), block)
        rows = pl.ds(pl.multiple_of(start + b * block, block), block)
        cosine, sine = cos_ref[here, :], sin_ref[here, :]
        q = rotated(pairs[rows, pl.ds(0, DK)].astype(jnp.float32), cosine, sine)
        q = q.astype(jnp.bfloat16)
        k = rotated(pairs[rows, pl.ds(DK, DK)].astype(jnp.float32), cosine, sine) * DK ** (-0.5)
        k = k.astype(jnp.bfloat16)
        scores = lax.dot_general(
            q, k, (((1,), (1,)), ((), ())), preferred_element_type=jnp.float32
        )
        pairs[rows, pl.ds(0, DK)] = q
        weights[rows, :] = (scores * inside[...]).astype(jnp.bfloat16)
        decayed[rows, :] = (k.astype(jnp.float32) * key_decay[:, 0:1]).astype(jnp.bfloat16)


def retain_blocks(start, length, tables, gain, held, memory, head_out):
    pairs, weights, decayed, values = held
    inside, query_decay = tables[2], tables[3]
    block = inside.shape[-1]
    block_decay = head_rate(float(block), power=True)
    memory[...] = jnp.zeros_like(memory)

    @pl.loop(0, length // block)
    def _(b):
        rows = pl.ds(pl.multiple_of(start + b * block, block), block)
        v = values[rows, :]
        state = memory[...]
        kept = jnp.dot(weights[rows, :], v, preferred_element_type=jnp.float32) + query_decay[
            :, 0:1
        ] * jnp.dot(
            pairs[rows, pl.ds(0, DK)],
            state.astype(jnp.bfloat16),
            preferred_element_type=jnp.float32,
        )
        memory[...] = state * block_decay + lax.dot_general(
            decayed[rows, :], v, (((0,), (0,)), ((), ())), preferred_element_type=jnp.float32
        )
        scale = lax.rsqrt(jnp.mean(kept * kept, axis=-1, keepdims=True) + norm_eps)
        head_out[rows, :] = (kept * scale * gain[...]).astype(jnp.bfloat16)


def layer_kernel(depth, splits, along, *refs):
    args, refs = refs[:13], refs[13:]
    resid, mix_gain, query, key, value, head_gain, out_w, mlp_gain, gate, up, down, cos, sin = args
    out, refs = refs[0], refs[1:]
    fulls, others, refs = refs[:5], refs[5:10], refs[10:]
    pair_full, value_full, out_full, gate_up, down_full = fulls
    pair_other, value_other, out_other, gate_up_other, down_other = others
    x, gain_mix, gain_head, gain_mlp, cos_v, sin_v, middle_gate, middle_up, refs = (
        *refs[:8],
        refs[8:],
    )
    normed, both, pairs, values, weights, decayed, memory, head_out, hidden, refs = (
        *refs[:9],
        refs[9:],
    )
    part, sent, got, far_part, far_sent, far_got, far_sum, far_in, middle, refs = (
        *refs[:9],
        refs[9:],
    )
    inside, query_decay, key_decay, refs = *refs[:3], refs[3:]
    send_sem, recv_sem, cross_send, cross_recv, refs = *refs[:4], refs[4:]
    load_sem, peer_send, peer_recv, beside_send, beside_recv = refs

    axes = (0, 0, 1, 0, 1)
    ga = Gather(
        depth,
        [Weight(*given) for given in zip(fulls, others, axes)],
        along,
        (cross_send, cross_recv),
        (send_sem, recv_sem),
    )
    ga.greet()
    peer = Near("tp", peer_send, peer_recv)
    beside = Near("fs", beside_send, beside_recv)
    core = lax.axis_index("tp")
    fs = lax.axis_index("fs")
    y = lax.rem(fs, 2)
    rows, width = x.shape
    units = gate.shape[1]
    whole = units // 2 // TILE
    aligned = whole * TILE
    step = aligned + TILE
    cols_of = down.shape[1]

    def own(w):
        weight = ga.weights[w]
        return ga.place(w, fs, 0, weight.rows)

    shard = query.shape[0]
    own_rows = pl.ds(pl.multiple_of(fs * shard, 16), shard)
    own_cols = pl.ds(pl.multiple_of(fs * cols_of, 128), cols_of)

    def heads(ref, side, size):
        return ref.at[:, pl.ds(pl.multiple_of(side * size, 128), size)]

    def down_pieces(side, place):
        rest = units // 2 - aligned
        return [
            (down.at[pl.ds(pl.multiple_of(side * step, 16), aligned), :], place(0, aligned)),
            (
                down.at[pl.ds(pl.multiple_of(aligned + side * rest, 16), rest), :],
                place(aligned, rest),
            ),
        ]

    moves = [
        (heads(query, y, DK), pair_full.at[own_rows, pl.ds(0, DK)]),
        (heads(key, y, DK), pair_full.at[own_rows, pl.ds(DK, DK)]),
        (heads(query, 1 - y, DK), pair_other.at[:, pl.ds(0, DK)]),
        (heads(key, 1 - y, DK), pair_other.at[:, pl.ds(DK, DK)]),
        (heads(value, y, DV), own(1)),
        (heads(value, 1 - y, DV), value_other),
        (resid, x),
        (mix_gain, gain_mix),
        (out_w.at[pl.ds(pl.multiple_of(y * DV, 16), DV), :], own(2)),
        (out_w.at[pl.ds(pl.multiple_of((1 - y) * DV, 16), DV), :], out_other),
        (gate.at[:, pl.ds(aligned, TILE)], middle_gate),
        (up.at[:, pl.ds(aligned, TILE)], middle_up),
        *down_pieces(y, lambda start, count: down_full.at[pl.ds(start, count), own_cols]),
        *down_pieces(1 - y, lambda start, count: down_other.at[pl.ds(start, count), :]),
        (cos, cos_v),
        (sin, sin_v),
        (heads(head_gain, y, DV), gain_head),
        (mlp_gain, gain_mlp),
    ]
    loads = [
        pltpu.make_async_copy(source, place, load_sem.at[i])
        for i, (source, place) in enumerate(moves)
    ]
    for load in loads[:8]:
        load.start()
    gathers = []

    def load_rest():
        for load in loads[8:12]:
            load.start()
        for side, target, index in ((y, own(3), 0), (1 - y, gate_up_other, 1)):
            sem = load_sem.at[len(moves) + index]

            @pl.loop(0, whole)
            def _(j):
                cols = pl.ds(pl.multiple_of(side * step + j * TILE, TILE), TILE)
                for i, source in enumerate((gate, up)):
                    place = pl.ds(pl.multiple_of(j * 2 * TILE, TILE) + i * TILE, TILE)
                    pltpu.make_async_copy(source.at[:, cols], target.at[:, place], sem).start()

            bulk = target.at[:, pl.ds(0, 2 * aligned)]
            gathers.append(pltpu.make_async_copy(bulk, bulk, sem))
        for load in loads[12:]:
            load.start()

    ga.meet()

    waited = set()

    def once(name, waits):
        if name not in waited:
            waited.add(name)
            for wait in waits:
                wait()

    def loaded(*indices):
        for i in indices:
            once(("load", i), [loads[i].wait])

    def side_of(far):
        return 1 - y if far else y

    def chip_rows(far, of):
        return pl.ds(pl.multiple_of((side_of(far) * 2 + of) * rows, 16), rows)

    def chip_start(far):
        return pl.multiple_of(side_of(far) * 2 * rows, 16)

    def tokens(far):
        return pl.ds(chip_start(far), 2 * rows)

    streams = (normed, both)
    starts = [sum(splits[:i]) for i in range(len(splits))]

    def rows_at(layer, far, of, i):
        start = pl.multiple_of((side_of(far) * 2 + of) * rows + starts[i], 16)
        return streams[layer].at[pl.ds(start, splits[i]), :]

    def join_own(layer, i, of):
        place = rows_at(layer, 0, of, i)
        return peer.copy(i, place, place)

    def join_far(layer, i, of):
        place = rows_at(layer, 1, of, i)
        return peer.copy(len(splits) + i, place, place)

    def join_beside(layer, i, far):
        place = rows_at(layer, far, core, i)
        return beside.copy(i, place, place)

    def wide(rank):
        return pl.ds(pl.multiple_of(ga.near(rank) * 2 * cols_of, 128), 2 * cols_of)

    def part_rows(i):
        return pl.ds(starts[i], splits[i])

    def share(rank):
        cols = wide(rank)
        return peer.copy(2 * len(splits) + rank, sent.at[:, cols], got.at[:, cols])

    def swap_far(rank, i):
        here, cols = part_rows(i), wide(rank)
        index = 2 * len(splits) + (1 + i) * depth + rank
        return peer.copy(index, far_sent.at[here, cols], far_got.at[here, cols])

    def give(rank, i):
        here, cols = part_rows(i), wide(rank)
        index = len(splits) + i * depth + rank
        return beside.copy(index, far_sum.at[here, cols], far_in.at[here, cols])

    def spread(layer, i):
        join_beside(layer, i, 0).start()
        join_own(layer, i, core).start()

    def norm_mix():
        load_rest()
        loaded(6, 7)
        for i, count in enumerate(splits):

            @pl.loop(0, count // ROWS)
            def _(r):
                at = starts[i] + r * ROWS
                here = pl.ds(pl.multiple_of(at, ROWS), ROWS)
                there = pl.ds(pl.multiple_of((y * 2 + core) * rows + at, ROWS), ROWS)
                normed[there, :] = scaled_rows(x[here, :].astype(jnp.float32), gain_mix[...])

            spread(0, i)
        loaded(10, 11)
        half = TILE // 2
        low_gate = middle_gate[...].astype(jnp.float32)
        low_up = middle_up[...].astype(jnp.float32)
        first = jnp.concatenate([low_gate[:, :half], low_up[:, :half]], axis=1)
        second = jnp.concatenate([low_gate[:, half:], low_up[:, half:]], axis=1)
        end = pl.ds(2 * aligned, TILE)
        mine = jnp.where(y == 0, first, second)
        theirs = jnp.where(y == 0, second, first)
        gate_up[own_rows, end] = mine.astype(jnp.bfloat16)
        gate_up_other[:, end] = theirs.astype(jnp.bfloat16)
        make_tables(inside, query_decay, key_decay)

    ready = {
        0: (0, 1), 1: (2, 3), 2: (4,), 3: (5,), 4: (8,), 5: (9,), 6: (), 7: (), 8: (12, 13),
        9: (14, 15),
    }

    def prepared(s):
        loaded(*ready[s])
        if s in (6, 7):
            once(("gather", s), [gathers[s - 6].wait])

    def h(s, t):
        if t == 0 and s % 2 == 0:
            prepared(s)
        ga.arrive(s, t)

    def cross(s):
        prepared(s)
        ga.cross(s).start()

    def pass_on(layer, i):
        join_beside(layer, i, 1).wait_recv()
        if layer == 1:
            join_far(0, i, core).wait_send()
        join_far(layer, i, core).start()

    def gathered(w):
        once(
            ("weight", w),
            [
                functools.partial(ga.joined, 2 * w + far, rank)
                for rank in range(depth)
                for far in (0, 1)
            ],
        )

    def arrived(layer, far, i):
        join = join_far if far else join_own
        once(("rows", layer, far, i), [lambda: join(layer, i, 1 - core).wait_recv()])

    def far_span(of, i):
        return pl.ds(pl.multiple_of((side_of(1) * 2 + of) * rows + starts[i], 16), splits[i])

    def spans(layer, far, i):
        if far:
            arrived(layer, 1, i)
            return [far_span(of, i) for of in (0, 1)]
        for part in range(len(splits)):
            arrived(layer, 0, part)
        return [tokens(0)]

    def project(w, far, i, place):
        gathered(w)
        ranges = spans(0, far, i)
        full = fulls[w]

        @pl.loop(0, full.shape[1] // 256)
        def _(c):
            cols = pl.ds(pl.multiple_of(c * 256, 256), 256)
            for here in ranges:
                place[here, cols] = jnp.dot(
                    normed[here, :], full[:, cols], preferred_element_type=jnp.float32
                ).astype(jnp.bfloat16)

    tables = (cos_v, sin_v, inside, query_decay, key_decay)

    def pairs_of(far, i=None):
        project(0, far, i, pairs)

    def values_of(far, i=None):
        project(1, far, i, values)

    def weigh(far):
        loaded(16, 17)
        weigh_blocks(chip_start(far), 2 * rows, tables, pairs, weights, decayed)

    def retain(far):
        loaded(18, 19)
        held = (pairs, weights, decayed, values)
        retain_blocks(chip_start(far), 2 * rows, tables, gain_head, held, memory, head_out)

    lefts, rights = (head_out, hidden), (out_full, down_full)

    def product(layer, taken, rank, place, here):
        for i in range(2):
            start = pl.multiple_of((ga.near(rank) * 2 + i) * cols_of, 128)
            cols = pl.ds(start, cols_of)
            place[here, cols] = jnp.dot(
                lefts[layer][taken, :], rights[layer][:, cols], preferred_element_type=jnp.float32
            ).astype(jnp.bfloat16)

    def rank_joined(layer, rank):
        for far in (0, 1):
            s = (4, 8)[layer] + far
            once(("rank", s, rank), [functools.partial(ga.joined, s, rank)])

    def far_rank(layer, rank, i):
        here, cols = part_rows(i), wide(rank)
        rank_joined(layer, rank)
        if layer == 1:
            swap_far(rank, i).wait_send()
            give(rank, i).wait_send()
        product(layer, far_span(1 - core, i), rank, far_sent, here)
        swap_far(rank, i).start()
        product(layer, far_span(core, i), rank, far_part, here)
        swap_far(rank, i).wait_recv()
        total = far_part[here, cols].astype(jnp.float32) + far_got[here, cols].astype(jnp.float32)
        far_sum[here, cols] = total.astype(jnp.bfloat16)
        give(rank, i).start()

    def own_rank(layer, rank):
        everything = pl.ds(0, rows)
        rank_joined(layer, rank)
        product(layer, chip_rows(0, 1 - core), rank, sent, everything)
        share(rank).start()
        product(layer, chip_rows(0, core), rank, part, everything)

    def norm_mlp(i):
        if i == 0:
            for rank in range(depth):
                share(rank).wait()
        for rank in range(depth):
            give(rank, i).wait_recv()
        join_beside(0, i, 0).wait_send()
        join_own(0, i, core).wait_send()

        @pl.loop(0, splits[i] // ROWS)
        def _(r):
            at = starts[i] + r * ROWS
            here = pl.ds(pl.multiple_of(at, ROWS), ROWS)
            there = pl.ds(pl.multiple_of((y * 2 + core) * rows + at, ROWS), ROWS)
            total = part[here, :].astype(jnp.float32) + got[here, :].astype(jnp.float32)
            total = total + far_in[here, :].astype(jnp.float32)
            mid = (x[here, :].astype(jnp.float32) + total).astype(jnp.bfloat16)
            middle[here, :] = mid
            both[there, :] = scaled_rows(mid.astype(jnp.float32), gain_mlp[...])

        spread(1, i)

    def activate(ranges):
        @pl.loop(0, whole)
        def _(j):
            cols = pl.ds(pl.multiple_of(j * 2 * TILE, 2 * TILE), 2 * TILE)
            place = pl.ds(pl.multiple_of(j * TILE, TILE), TILE)
            for here in ranges:
                two = jnp.dot(both[here, :], gate_up[:, cols], preferred_element_type=jnp.float32)
                hidden[here, place] = (jax.nn.silu(two[:, :TILE]) * two[:, TILE:]).astype(
                    jnp.bfloat16
                )

        half = TILE // 2
        for here in ranges:
            two = jnp.dot(
                both[here, :],
                gate_up[:, pl.ds(2 * aligned, TILE)],
                preferred_element_type=jnp.float32,
            )
            hidden[here, pl.ds(aligned, half)] = (
                jax.nn.silu(two[:, :half]) * two[:, half:]
            ).astype(jnp.bfloat16)

    def expand(far, i=None):
        gathered(3)
        activate(spans(1, far, i))

    def drain():
        for s in range(2 * len(fulls)):
            ga.drain(s)
        for i in range(len(splits)):
            join_own(1, i, core).wait_send()
            join_far(1, i, core).wait_send()
            join_beside(1, i, 0).wait_send()

    def finish():
        drain()
        for rank in range(depth):
            share(rank).wait()
        writes = []
        for i in range(len(splits)):
            here = part_rows(i)
            for rank in range(depth):
                cols = wide(rank)
                give(rank, i).wait_recv()
                total = part[here, cols].astype(jnp.float32) + got[here, cols].astype(jnp.float32)
                total = total + far_in[here, cols].astype(jnp.float32)
                middle[here, cols] = (middle[here, cols].astype(jnp.float32) + total).astype(
                    jnp.bfloat16
                )
                write = pltpu.make_async_copy(
                    middle.at[here, cols], out.at[here, cols], load_sem.at[len(writes)]
                )
                write.start()
                writes.append(write)
        for rank in range(depth):
            for i in range(len(splits)):
                swap_far(rank, i).wait_send()
                give(rank, i).wait_send()
        for write in writes:
            write.wait()

    order = [
        (cross, 1), (h, 0, 0), (h, 2, 0), (cross, 3), (norm_mix,), (h, 1, 0), (h, 0, 1),
        (h, 1, 1), (h, 2, 1), (h, 1, 2), (h, 0, 2), (cross, 5), (h, 2, 2), (h, 1, 3), (h, 3, 0),
        (h, 4, 0), (h, 0, 3), (h, 3, 1), (h, 2, 3), (pass_on, 0, 0), (cross, 9), (pairs_of, 1, 0),
        (h, 3, 2), (h, 3, 3), (h, 4, 1), (pairs_of, 0), (cross, 7), (h, 4, 2), (pass_on, 0, 1),
        (h, 5, 0), (pairs_of, 1, 1), (values_of, 1, 1), (values_of, 1, 0), (weigh, 1), (h, 5, 1),
        (h, 4, 3), (retain, 1), (h, 6, 0), (far_rank, 0, 0, 1), (h, 5, 2), (far_rank, 0, 1, 0),
        (h, 7, 0), (weigh, 0), (values_of, 0), (far_rank, 0, 2, 0), (h, 5, 3),
        (far_rank, 0, 0, 0), (h, 6, 1), (retain, 0), (far_rank, 0, 3, 0), (far_rank, 0, 2, 1),
        (h, 7, 1), (own_rank, 0, 0), (own_rank, 0, 1), (own_rank, 0, 2), (far_rank, 0, 3, 1),
        (far_rank, 0, 1, 1), (own_rank, 0, 3), (h, 6, 2), (norm_mlp, 0), (h, 7, 2), (h, 6, 3),
        (h, 8, 0), (h, 7, 3), (norm_mlp, 1), (h, 9, 0), (h, 8, 1), (pass_on, 1, 0), (h, 9, 1),
        (expand, 1, 0), (h, 8, 2), (far_rank, 1, 0, 0), (pass_on, 1, 1), (h, 9, 2),
        (far_rank, 1, 1, 0), (expand, 1, 1), (far_rank, 1, 0, 1), (far_rank, 1, 2, 0), (h, 8, 3),
        (far_rank, 1, 1, 1), (h, 9, 3), (far_rank, 1, 2, 1), (expand, 0), (far_rank, 1, 3, 0),
        (far_rank, 1, 3, 1), (own_rank, 1, 0), (own_rank, 1, 1), (own_rank, 1, 3),
        (own_rank, 1, 2), (finish,),
    ]
    for job, *given in order:
        job(*given)


def rotation_tables(length_total, half_width):
    position = np.arange(length_total, dtype=np.float32)
    inverse = (1.0 / rope_base ** np.linspace(0.0, 1.0, half_width)).astype(np.float32)
    angle = (position[:, None] * inverse[None, :]).astype(np.float64)
    return np.cos(angle).astype(np.float32), np.sin(angle).astype(np.float32)


def fits(rows, width, key_cols, value_cols, units, shard, out_cols):
    axes = lax.axis_size("rep") == 2 and lax.axis_size("fs") == 8 and lax.axis_size("tp") == 2
    cut = units % (2 * TILE) == TILE and (units // 2) % 32 == 0
    whole = width == 8 * out_cols and width == 8 * shard and shard % 256 == 0
    heads = key_cols == 2 * DK and value_cols == 2 * DV
    return axes and cut and whole and heads and rows % 192 == 0


def layer(args):
    resid, query, gate, down = args[0], args[2], args[8], args[10]
    size = lax.axis_size("fs")
    depth = size // 2
    rows, width = resid.shape
    tokens = 4 * rows
    units = gate.shape[1]
    shard, out_cols = query.shape[0], down.shape[1]
    others = [(shard, 2 * DK), (shard, DV), (DV, out_cols), (shard, units), (units // 2, out_cols)]
    fulls = []
    for (r, c), axis in zip(others, (0, 0, 1, 0, 1)):
        fulls.append((r * size, c) if axis == 0 else (r, c * size))
    along = [shard // 2, shard // 16 * 9 // 16 * 16, DV // 16 * 18 // 32 * 16, shard // 2, units // 2 // 16 * 30 // 44 * 16]
    splits = (2 * rows // 3, rows // 3)
    cosine, sine = rotation_tables(2 * rows, DK // 2)
    far = pl.BlockSpec(memory_space=pl.ANY)
    bf, f32 = jnp.bfloat16, jnp.float32
    vm = pltpu.VMEM
    dma = pltpu.SemaphoreType.DMA
    slices = 2 * len(fulls)
    peers = 2 * len(splits) + (1 + len(splits)) * depth
    args = [a[None, :] if a.ndim == 1 else a for a in args]
    return pl.pallas_call(
        functools.partial(layer_kernel, depth, splits, along),
        out_shape=jax.ShapeDtypeStruct((rows, width), bf),
        in_specs=[far] * 13,
        out_specs=far,
        scratch_shapes=[vm(s, bf) for s in fulls]
        + [vm(s, bf) for s in others]
        + [
            vm((rows, width), bf),
            vm(args[1].shape, f32),
            vm((1, DV), f32),
            vm(args[7].shape, f32),
            vm(cosine.shape, f32),
            vm(sine.shape, f32),
            vm((shard, TILE), bf),
            vm((shard, TILE), bf),
            vm((tokens, width), bf),
            vm((tokens, width), bf),
            vm((tokens, 2 * DK), bf),
            vm((tokens, DV), bf),
            vm((tokens, BLOCK), bf),
            vm((tokens, DK), bf),
            vm((DK, DV), f32),
            vm((tokens, DV), bf),
            vm((tokens, units // 2), bf),
        ]
        + [vm((rows, width), bf)] * 9
        + [vm((BLOCK, BLOCK), f32)] * 3
        + [
            dma((slices, 2 * depth + 1)),
            dma((slices, 2 * depth)),
            dma((len(fulls),)),
            dma((len(fulls),)),
            dma((22,)),
            dma((peers,)),
            dma((peers,)),
            dma((len(splits) * (1 + depth),)),
            dma((len(splits) * (1 + depth),)),
        ],
        compiler_params=pltpu.CompilerParams(
            collective_id=0, has_side_effects=True, vmem_limit_bytes=67043328
        ),
    )(*args, jnp.asarray(cosine), jnp.asarray(sine))


DK = 256
DV = 512
BLOCK = 128


norm_eps = 1e-06
rope_base = 10000.0


def rms_scale(values, gain):
    widened = values.astype(jnp.float32)
    scaled = widened * lax.rsqrt(jnp.mean(widened * widened, axis=-1, keepdims=True) + norm_eps)
    return (scaled * gain).astype(jnp.bfloat16)


def rotation(length_total, half_width):
    position = jnp.arange(length_total, dtype=jnp.float32)
    inverse = 1.0 / rope_base ** jnp.linspace(0.0, 1.0, half_width, dtype=jnp.float32)
    angle = position[:, None] * inverse[None, :]
    return (jnp.cos(angle), jnp.sin(angle))


def rotate(vectors):
    length_total = vectors.shape[0]
    half_width = vectors.shape[-1] // 2
    cosine, sine = rotation(length_total, half_width)
    cosine, sine = cosine[:, None, :], sine[:, None, :]
    first = vectors[..., :half_width]
    second = vectors[..., half_width:]
    return jnp.concatenate(
        [first * cosine - second * sine, second * cosine + first * sine], axis=-1
    )


def decay_tables(head_ids, block):
    log_gamma = jnp.log1p(-(2.0 ** (-5.0 - 2.0 * head_ids.astype(jnp.float32))))
    offset = jnp.arange(block, dtype=jnp.float32)
    distance = offset[:, None] - offset[None, :]
    inside = jnp.where(
        distance >= 0, jnp.exp(log_gamma[:, None, None] * jnp.maximum(distance, 0.0)), 0.0
    )
    query_decay = jnp.exp(log_gamma[:, None] * (offset + 1.0))
    key_decay = jnp.exp(log_gamma[:, None] * (block - 1.0 - offset))
    block_decay = jnp.exp(log_gamma * block)
    return (inside, query_decay, key_decay, block_decay)


def retain(queries, keys, values, head_ids, block):
    length_total, heads, key_width = queries.shape
    value_width = values.shape[-1]
    count = length_total // block
    inside, query_decay, key_decay, block_decay = decay_tables(head_ids, block)

    def blocks(tensor):
        return tensor.reshape(count, block, heads, tensor.shape[-1]).transpose(0, 2, 1, 3)

    def advance(memory, inputs):
        query_tile_rows, key_tile_rows, value_block = inputs
        attention_scores = jnp.einsum(
            "zvf,zjf->zvj", query_tile_rows, key_tile_rows, preferred_element_type=jnp.float32
        )
        weights = (attention_scores * inside).astype(jnp.bfloat16)
        within = jnp.einsum(
            "hlm,hmv->hlv", weights, value_block, preferred_element_type=jnp.float32
        )
        carried = (
            jnp.einsum(
                "hld,hdv->hlv",
                query_tile_rows,
                memory.astype(jnp.bfloat16),
                preferred_element_type=jnp.float32,
            )
            * query_decay[:, :, None]
        )
        weighted_keys = (key_tile_rows.astype(jnp.float32) * key_decay[:, :, None]).astype(
            jnp.bfloat16
        )
        memory = memory * block_decay[:, None, None] + jnp.einsum(
            "hld,hlv->hdv", weighted_keys, value_block, preferred_element_type=jnp.float32
        )
        return (memory, within + carried)

    start_state = jnp.zeros((heads, key_width, value_width), jnp.float32)
    _, outputs = lax.scan(advance, start_state, (blocks(queries), blocks(keys), blocks(values)))
    return outputs.transpose(0, 2, 1, 3).reshape(length_total, heads, value_width)


def head_scale(retained, gain):
    scaled = retained * lax.rsqrt(jnp.mean(retained * retained, axis=-1, keepdims=True) + norm_eps)
    return (scaled.reshape(retained.shape[0], -1) * gain).astype(jnp.bfloat16)


def swap(rows):
    return lax.ppermute(rows, "tp", [(0, 1), (1, 0)])


def join_rows(rows):
    if lax.axis_size("tp") != 2:
        return lax.all_gather(rows, "tp", axis=0, tiled=True)
    first = lax.axis_index("tp") == 0
    got = swap(rows)
    return jnp.concatenate([jnp.where(first, rows, got), jnp.where(first, got, rows)], axis=0)


def share_sum(part):
    if lax.axis_size("tp") != 2:
        summed = lax.psum_scatter(part, "tp", scatter_dimension=0, tiled=True)
        return summed.astype(jnp.float32)
    count = part.shape[0] // 2
    me = lax.axis_index("tp")
    mine = lax.dynamic_slice_in_dim(part, me * count, count, axis=0)
    theirs = lax.dynamic_slice_in_dim(part, (1 - me) * count, count, axis=0)
    return mine.astype(jnp.float32) + swap(theirs).astype(jnp.float32)


def shards(
    resid,
    mix_gain,
    query_weight,
    key_weight,
    value_weight,
    head_gain,
    out_weight,
    mlp_gain,
    gate_weight,
    up_weight,
    down_weight,
):
    token_rows = resid.shape[0]
    length_total = token_rows * lax.axis_size("tp")
    key_cols = query_weight.shape[1]
    heads_here = key_cols // DK
    sizes = (
        token_rows, resid.shape[1], key_cols, value_weight.shape[1], gate_weight.shape[1],
        query_weight.shape[0], down_weight.shape[1],
    )
    if fits(*sizes):
        args = [
            resid, mix_gain, query_weight, key_weight, value_weight, head_gain,
            out_weight, mlp_gain, gate_weight, up_weight, down_weight,
        ]
        return layer(args)
    normed = rms_scale(resid, mix_gain)
    mixer_shard = jnp.concatenate([query_weight, key_weight, value_weight], axis=1)
    mlp_shard = jnp.concatenate([gate_weight, up_weight], axis=1)
    normed_full = join_rows(normed)
    head_ids = lax.axis_index("tp") * heads_here + jnp.arange(heads_here, dtype=jnp.int32)
    pieces = [mixer_shard, out_weight, mlp_shard, down_weight]
    mixer_full, out_full, mlp_full, down_full = (
        lax.all_gather(s, "fs", axis=a, tiled=True) for s, a in zip(pieces, [0, 1, 0, 1])
    )
    projected = jnp.dot(
        normed_full, mixer_full, preferred_element_type=jnp.float32
    ).astype(jnp.bfloat16)
    both_keys = projected[:, : 2 * key_cols].astype(jnp.float32)
    both_keys = both_keys.reshape(length_total, 2, heads_here, DK)
    values = projected[:, 2 * key_cols :].reshape(length_total, heads_here, DV)
    query_rot = rotate(both_keys[:, 0]).astype(jnp.bfloat16)
    key_rot = (rotate(both_keys[:, 1]) * DK ** (-0.5)).astype(jnp.bfloat16)
    retained = retain(query_rot, key_rot, values, head_ids, BLOCK)
    head_out = head_scale(retained, head_gain)
    part = jnp.dot(head_out, out_full, preferred_element_type=jnp.float32).astype(jnp.bfloat16)
    mixer_sum = share_sum(part)
    middle = (resid.astype(jnp.float32) + mixer_sum).astype(jnp.bfloat16)
    normed_mlp = rms_scale(middle, mlp_gain)
    local_units = gate_weight.shape[1]
    both = jnp.dot(
        join_rows(normed_mlp),
        mlp_full,
        preferred_element_type=jnp.float32,
    )
    hidden_units = (jax.nn.silu(both[:, :local_units]) * both[:, local_units:]).astype(jnp.bfloat16)
    mlp_sum = share_sum(
        jnp.dot(hidden_units, down_full, preferred_element_type=jnp.float32).astype(jnp.bfloat16)
    )
    return (middle.astype(jnp.float32) + mlp_sum).astype(jnp.bfloat16)


def solution(mesh):
    placed = (
        P(("rep", "fs", "tp"), None),
        P(),
        P("fs", "tp"),
        P("fs", "tp"),
        P("fs", "tp"),
        P("tp"),
        P("tp", "fs"),
        P(),
        P("fs", "tp"),
        P("fs", "tp"),
        P("tp", "fs"),
    )
    return jax.shard_map(
        shards, mesh=mesh, in_specs=placed, out_specs=P(("rep", "fs", "tp"), None), check_vma=False
    )
```

```python
import functools
import math

import jax
import jax.numpy as jnp
import numpy as np
from jax import lax
from jax.experimental import pallas as pl
from jax.experimental.pallas import tpu as pltpu
from jax.sharding import PartitionSpec as P

MESH = pl.DeviceIdType.MESH
ROWS = 64
TILE = 128


class Weight:
    def __init__(self, full, other, axis):
        self.full, self.other, self.axis = full, other, axis
        self.rows, self.cols = other.shape


class Gather:
    def __init__(self, depth, weights, along, cross_sems, sems):
        self.depth, self.weights, self.along = depth, weights, along
        self.cross_send, self.cross_recv = cross_sems
        self.send_sem, self.recv_sem = sems
        self.x = lax.axis_index("rep")
        fs = lax.axis_index("fs")
        self.z = fs // 2
        self.y = lax.rem(fs, 2)

    def greet(self):
        sem = pltpu.get_barrier_semaphore()
        z, y, x = self.z, self.y, self.x
        core = lax.axis_index("tp")
        pl.semaphore_signal(sem, inc=1, device_id={"tp": 1 - core}, device_id_type=MESH)
        pl.semaphore_signal(sem, inc=1, device_id={"rep": 1 - x}, device_id_type=MESH)
        pl.semaphore_signal(sem, inc=1, device_id={"fs": z * 2 + 1 - y}, device_id_type=MESH)

        @pl.when(z > 0)
        def _():
            pl.semaphore_signal(sem, inc=1, device_id={"fs": (z - 1) * 2 + y}, device_id_type=MESH)

        @pl.when(z < self.depth - 1)
        def _():
            pl.semaphore_signal(sem, inc=1, device_id={"fs": (z + 1) * 2 + y}, device_id_type=MESH)

    def meet(self):
        low = jnp.minimum(self.z, 1)
        high = jnp.minimum(self.depth - 1 - self.z, 1)
        pl.semaphore_wait(pltpu.get_barrier_semaphore(), 3 + low + high)

    def near(self, rank):
        place = 0
        for z in range(self.depth):
            order = sorted(range(self.depth), key=lambda other: (abs(other - z), other))
            place = place + order[rank] * jnp.where(self.z == z, 1, 0)
        return place

    def block(self, far, origin):
        return origin * 2 + (1 - self.y if far else self.y)

    def place(self, w, block, start, count):
        weight = self.weights[w]
        if weight.axis == 0:
            first = pl.multiple_of(block * weight.rows + start, 16)
            return weight.full.at[pl.ds(first, count), :]
        cols = pl.ds(pl.multiple_of(block * weight.cols, 128), weight.cols)
        return weight.full.at[pl.ds(pl.multiple_of(start, 16), count), cols]

    def cross(self, s, incoming=False):
        w = s // 2
        count = self.along[w]
        start = pl.multiple_of((self.weights[w].rows - count) * self.x, 16)
        block = self.z * 2 + (1 - self.y if incoming else self.y)
        return pltpu.make_async_remote_copy(
            src_ref=self.weights[w].other.at[pl.ds(start, count), :],
            dst_ref=self.place(w, block, start, count),
            send_sem=self.cross_send.at[w],
            recv_sem=self.cross_recv.at[w],
            device_id={"fs": self.z * 2 + 1 - self.y},
            device_id_type=MESH,
        )

    def copy(self, s, kind, origin, incoming=False, own=False):
        w, far = s // 2, s % 2
        x, y, z = self.x, self.y, self.z
        rows, along = self.weights[w].rows, self.along[w]
        if kind == "x":
            count = rows - along
            start = along * (1 - x if incoming else x)
        else:
            count = along
            start = (rows - along) * x
        target = {
            "up": {"fs": (z + 1) * 2 + y},
            "down": {"fs": (z - 1) * 2 + y},
            "x": {"rep": 1 - x},
        }[kind]
        place = self.place(w, self.block(far, origin), start, count)
        slot = origin
        if kind == "x":
            slot = self.depth + origin
        elif kind == "down" and own:
            slot = 2 * self.depth
        return pltpu.make_async_remote_copy(
            src_ref=place,
            dst_ref=place,
            send_sem=self.send_sem.at[s, slot],
            recv_sem=self.recv_sem.at[s, origin + (self.depth if kind == "x" else 0)],
            device_id=target,
            device_id_type=MESH,
        )

    def each(self, t, body):
        if t == 0:
            body("own", self.z)
            return

        @pl.when(self.z - t >= 0)
        def _():
            body("up", self.z - t)

        @pl.when(self.z + t < self.depth)
        def _():
            body("down", self.z + t)

    def onward(self, s, way, origin, act):
        if way in ("own", "up"):

            @pl.when(self.z < self.depth - 1)
            def _():
                act(self.copy(s, "up", origin))

        if way in ("own", "down"):

            @pl.when(self.z > 0)
            def _():
                act(self.copy(s, "down", origin, own=way == "own"))

    def arrive(self, s, t):
        def body(way, origin):
            if way != "own":
                self.copy(s, way, origin, incoming=True).wait_recv()
            elif s % 2:
                self.cross(s, incoming=True).wait_recv()
            self.onward(s, way, origin, lambda c: c.start())
            if way != "own" or s % 2:
                self.copy(s, "x", origin).start()

        self.each(t, body)

    def joined(self, s, rank):
        if rank > 0 or s % 2:
            self.copy(s, "x", self.near(rank), incoming=True).wait_recv()

    def drain(self, s):
        for back in range(self.depth):

            def sent(way, origin):
                self.onward(s, way, origin, lambda c: c.wait_send())
                if way != "own" or s % 2:
                    self.copy(s, "x", origin).wait_send()

            self.each(back, sent)
        if s % 2:
            self.cross(s).wait_send()


class Near:
    def __init__(self, axis, send_sem, recv_sem):
        self.send_sem, self.recv_sem = send_sem, recv_sem
        if axis == "tp":
            self.target = {"tp": 1 - lax.axis_index("tp")}
        else:
            fs = lax.axis_index("fs")
            self.target = {"fs": fs // 2 * 2 + 1 - lax.rem(fs, 2)}

    def copy(self, index, source, place):
        return pltpu.make_async_remote_copy(
            src_ref=source,
            dst_ref=place,
            send_sem=self.send_sem.at[index],
            recv_sem=self.recv_sem.at[index],
            device_id=self.target,
            device_id_type=MESH,
        )


def rotated(v, cosine, sine):
    half = v.shape[-1] // 2
    first, second = v[:, :half], v[:, half:]
    return jnp.concatenate(
        [first * cosine - second * sine, second * cosine + first * sine], axis=-1
    )


def scaled_rows(values, gain):
    scale = lax.rsqrt(jnp.mean(values * values, axis=-1, keepdims=True) + norm_eps)
    return (values * scale * gain).astype(jnp.bfloat16)


def head_rate(scale, power=False):
    core = lax.axis_index("tp")
    y = lax.rem(lax.axis_index("fs"), 2)
    rates = [scale * math.log1p(-(2.0 ** (-5.0 - 2.0 * i))) for i in range(4)]
    if power:
        rates = [math.exp(r) for r in rates]
    return jnp.where(
        core == 0,
        jnp.where(y == 0, rates[0], rates[1]),
        jnp.where(y == 0, rates[2], rates[3]),
    )


def make_tables(inside, query_decay, key_decay):
    block = inside.shape[-1]
    row = lax.broadcasted_iota(jnp.int32, (block, block), 0).astype(jnp.float32)
    col = lax.broadcasted_iota(jnp.int32, (block, block), 1).astype(jnp.float32)
    distance = row - col
    rate = head_rate(1.0)
    inside[...] = jnp.where(distance >= 0, jnp.exp(rate * jnp.maximum(distance, 0.0)), 0.0)
    query_decay[...] = jnp.exp(rate * (row + 1.0))
    key_decay[...] = jnp.exp(rate * (block - 1.0 - row))


def weigh_blocks(start, length, tables, pairs, weights, decayed):
    cos_ref, sin_ref, inside, _, key_decay = tables
    block = inside.shape[-1]

    @pl.loop(0, length // block)
    def _(b):
        here = pl.ds(pl.multiple_of(b * block, block), block)
        rows = pl.ds(pl.multiple_of(start + b * block, block), block)
        cosine, sine = cos_ref[here, :], sin_ref[here, :]
        q = rotated(pairs[rows, pl.ds(0, DK)].astype(jnp.float32), cosine, sine)
        q = q.astype(jnp.bfloat16)
        k = rotated(pairs[rows, pl.ds(DK, DK)].astype(jnp.float32), cosine, sine) * DK ** (-0.5)
        k = k.astype(jnp.bfloat16)
        scores = lax.dot_general(
            q, k, (((1,), (1,)), ((), ())), preferred_element_type=jnp.float32
        )
        pairs[rows, pl.ds(0, DK)] = q
        weights[rows, :] = (scores * inside[...]).astype(jnp.bfloat16)
        decayed[rows, :] = (k.astype(jnp.float32) * key_decay[:, 0:1]).astype(jnp.bfloat16)


def retain_blocks(start, length, tables, gain, held, memory, head_out):
    pairs, weights, decayed, values = held
    inside, query_decay = tables[2], tables[3]
    block = inside.shape[-1]
    block_decay = head_rate(float(block), power=True)
    memory[...] = jnp.zeros_like(memory)

    @pl.loop(0, length // block)
    def _(b):
        rows = pl.ds(pl.multiple_of(start + b * block, block), block)
        v = values[rows, :]
        state = memory[...]
        kept = jnp.dot(weights[rows, :], v, preferred_element_type=jnp.float32) + query_decay[
            :, 0:1
        ] * jnp.dot(
            pairs[rows, pl.ds(0, DK)],
            state.astype(jnp.bfloat16),
            preferred_element_type=jnp.float32,
        )
        memory[...] = state * block_decay + lax.dot_general(
            decayed[rows, :], v, (((0,), (0,)), ((), ())), preferred_element_type=jnp.float32
        )
        scale = lax.rsqrt(jnp.mean(kept * kept, axis=-1, keepdims=True) + norm_eps)
        head_out[rows, :] = (kept * scale * gain[...]).astype(jnp.bfloat16)


def layer_kernel(depth, splits, along, *refs):
    args, refs = refs[:13], refs[13:]
    resid, mix_gain, query, key, value, head_gain, out_w, mlp_gain, gate, up, down, cos, sin = args
    out, refs = refs[0], refs[1:]
    fulls, others, refs = refs[:5], refs[5:10], refs[10:]
    pair_full, value_full, out_full, gate_up, down_full = fulls
    pair_other, value_other, out_other, gate_up_other, down_other = others
    x, gain_mix, gain_head, gain_mlp, cos_v, sin_v, middle_gate, middle_up, refs = (
        *refs[:8],
        refs[8:],
    )
    normed, both, pairs, values, weights, decayed, memory, head_out, hidden, refs = (
        *refs[:9],
        refs[9:],
    )
    part, sent, got, far_part, far_sent, far_got, far_sum, far_in, middle, refs = (
        *refs[:9],
        refs[9:],
    )
    inside, query_decay, key_decay, refs = *refs[:3], refs[3:]
    send_sem, recv_sem, cross_send, cross_recv, refs = *refs[:4], refs[4:]
    load_sem, peer_send, peer_recv, beside_send, beside_recv = refs

    axes = (0, 0, 1, 0, 1)
    ga = Gather(
        depth,
        [Weight(*given) for given in zip(fulls, others, axes)],
        along,
        (cross_send, cross_recv),
        (send_sem, recv_sem),
    )
    ga.greet()
    peer = Near("tp", peer_send, peer_recv)
    beside = Near("fs", beside_send, beside_recv)
    core = lax.axis_index("tp")
    fs = lax.axis_index("fs")
    y = lax.rem(fs, 2)
    rows, width = x.shape
    units = gate.shape[1]
    whole = units // 2 // TILE
    aligned = whole * TILE
    step = aligned + TILE
    cols_of = down.shape[1]

    def own(w):
        weight = ga.weights[w]
        return ga.place(w, fs, 0, weight.rows)

    shard = query.shape[0]
    own_rows = pl.ds(pl.multiple_of(fs * shard, 16), shard)
    own_cols = pl.ds(pl.multiple_of(fs * cols_of, 128), cols_of)

    def heads(ref, side, size):
        return ref.at[:, pl.ds(pl.multiple_of(side * size, 128), size)]

    def down_pieces(side, place):
        rest = units // 2 - aligned
        return [
            (down.at[pl.ds(pl.multiple_of(side * step, 16), aligned), :], place(0, aligned)),
            (
                down.at[pl.ds(pl.multiple_of(aligned + side * rest, 16), rest), :],
                place(aligned, rest),
            ),
        ]

    moves = [
        (heads(query, y, DK), pair_full.at[own_rows, pl.ds(0, DK)]),
        (heads(key, y, DK), pair_full.at[own_rows, pl.ds(DK, DK)]),
        (heads(query, 1 - y, DK), pair_other.at[:, pl.ds(0, DK)]),
        (heads(key, 1 - y, DK), pair_other.at[:, pl.ds(DK, DK)]),
        (heads(value, y, DV), own(1)),
        (heads(value, 1 - y, DV), value_other),
        (resid, x),
        (mix_gain, gain_mix),
        (out_w.at[pl.ds(pl.multiple_of(y * DV, 16), DV), :], own(2)),
        (out_w.at[pl.ds(pl.multiple_of((1 - y) * DV, 16), DV), :], out_other),
        (gate.at[:, pl.ds(aligned, TILE)], middle_gate),
        (up.at[:, pl.ds(aligned, TILE)], middle_up),
        *down_pieces(y, lambda start, count: down_full.at[pl.ds(start, count), own_cols]),
        *down_pieces(1 - y, lambda start, count: down_other.at[pl.ds(start, count), :]),
        (cos, cos_v),
        (sin, sin_v),
        (heads(head_gain, y, DV), gain_head),
        (mlp_gain, gain_mlp),
    ]
    loads = [
        pltpu.make_async_copy(source, place, load_sem.at[i])
        for i, (source, place) in enumerate(moves)
    ]
    for load in loads[:8]:
        load.start()
    gathers = []

    def load_rest():
        for load in loads[8:12]:
            load.start()
        for side, target, index in ((y, own(3), 0), (1 - y, gate_up_other, 1)):
            sem = load_sem.at[len(moves) + index]

            @pl.loop(0, whole)
            def _(j):
                cols = pl.ds(pl.multiple_of(side * step + j * TILE, TILE), TILE)
                for i, source in enumerate((gate, up)):
                    place = pl.ds(pl.multiple_of(j * 2 * TILE, TILE) + i * TILE, TILE)
                    pltpu.make_async_copy(source.at[:, cols], target.at[:, place], sem).start()

            bulk = target.at[:, pl.ds(0, 2 * aligned)]
            gathers.append(pltpu.make_async_copy(bulk, bulk, sem))
        for load in loads[12:]:
            load.start()

    ga.meet()

    waited = set()

    def once(name, waits):
        if name not in waited:
            waited.add(name)
            for wait in waits:
                wait()

    def loaded(*indices):
        for i in indices:
            once(("load", i), [loads[i].wait])

    def side_of(far):
        return 1 - y if far else y

    def chip_rows(far, of):
        return pl.ds(pl.multiple_of((side_of(far) * 2 + of) * rows, 16), rows)

    def chip_start(far):
        return pl.multiple_of(side_of(far) * 2 * rows, 16)

    def tokens(far):
        return pl.ds(chip_start(far), 2 * rows)

    streams = (normed, both)
    starts = [sum(splits[:i]) for i in range(len(splits))]

    def rows_at(layer, far, of, i):
        start = pl.multiple_of((side_of(far) * 2 + of) * rows + starts[i], 16)
        return streams[layer].at[pl.ds(start, splits[i]), :]

    def join_own(layer, i, of):
        place = rows_at(layer, 0, of, i)
        return peer.copy(i, place, place)

    def join_far(layer, i, of):
        place = rows_at(layer, 1, of, i)
        return peer.copy(len(splits) + i, place, place)

    def join_beside(layer, i, far):
        place = rows_at(layer, far, core, i)
        return beside.copy(i, place, place)

    def wide(rank):
        return pl.ds(pl.multiple_of(ga.near(rank) * 2 * cols_of, 128), 2 * cols_of)

    def part_rows(i):
        return pl.ds(starts[i], splits[i])

    def share(rank):
        cols = wide(rank)
        return peer.copy(2 * len(splits) + rank, sent.at[:, cols], got.at[:, cols])

    def swap_far(rank, i):
        here, cols = part_rows(i), wide(rank)
        index = 2 * len(splits) + (1 + i) * depth + rank
        return peer.copy(index, far_sent.at[here, cols], far_got.at[here, cols])

    def give(rank, i):
        here, cols = part_rows(i), wide(rank)
        index = len(splits) + i * depth + rank
        return beside.copy(index, far_sum.at[here, cols], far_in.at[here, cols])

    def spread(layer, i):
        join_beside(layer, i, 0).start()
        join_own(layer, i, core).start()

    def norm_mix():
        load_rest()
        loaded(6, 7)
        for i, count in enumerate(splits):

            @pl.loop(0, count // ROWS)
            def _(r):
                at = starts[i] + r * ROWS
                here = pl.ds(pl.multiple_of(at, ROWS), ROWS)
                there = pl.ds(pl.multiple_of((y * 2 + core) * rows + at, ROWS), ROWS)
                normed[there, :] = scaled_rows(x[here, :].astype(jnp.float32), gain_mix[...])

            spread(0, i)
        loaded(10, 11)
        half = TILE // 2
        low_gate = middle_gate[...].astype(jnp.float32)
        low_up = middle_up[...].astype(jnp.float32)
        first = jnp.concatenate([low_gate[:, :half], low_up[:, :half]], axis=1)
        second = jnp.concatenate([low_gate[:, half:], low_up[:, half:]], axis=1)
        end = pl.ds(2 * aligned, TILE)
        mine = jnp.where(y == 0, first, second)
        theirs = jnp.where(y == 0, second, first)
        gate_up[own_rows, end] = mine.astype(jnp.bfloat16)
        gate_up_other[:, end] = theirs.astype(jnp.bfloat16)
        make_tables(inside, query_decay, key_decay)

    ready = {
        0: (0, 1), 1: (2, 3), 2: (4,), 3: (5,), 4: (8,), 5: (9,), 6: (), 7: (), 8: (12, 13),
        9: (14, 15),
    }

    def prepared(s):
        loaded(*ready[s])
        if s in (6, 7):
            once(("gather", s), [gathers[s - 6].wait])

    def h(s, t):
        if t == 0 and s % 2 == 0:
            prepared(s)
        ga.arrive(s, t)

    def cross(s):
        prepared(s)
        ga.cross(s).start()

    def pass_on(layer, i):
        join_beside(layer, i, 1).wait_recv()
        if layer == 1:
            join_far(0, i, core).wait_send()
        join_far(layer, i, core).start()

    def gathered(w):
        once(
            ("weight", w),
            [
                functools.partial(ga.joined, 2 * w + far, rank)
                for rank in range(depth)
                for far in (0, 1)
            ],
        )

    def arrived(layer, far, i):
        join = join_far if far else join_own
        once(("rows", layer, far, i), [lambda: join(layer, i, 1 - core).wait_recv()])

    def far_span(of, i):
        return pl.ds(pl.multiple_of((side_of(1) * 2 + of) * rows + starts[i], 16), splits[i])

    def spans(layer, far, i):
        if far:
            arrived(layer, 1, i)
            return [far_span(of, i) for of in (0, 1)]
        for part in range(len(splits)):
            arrived(layer, 0, part)
        return [tokens(0)]

    def project(w, far, i, place):
        gathered(w)
        ranges = spans(0, far, i)
        full = fulls[w]

        @pl.loop(0, full.shape[1] // 256)
        def _(c):
            cols = pl.ds(pl.multiple_of(c * 256, 256), 256)
            for here in ranges:
                place[here, cols] = jnp.dot(
                    normed[here, :], full[:, cols], preferred_element_type=jnp.float32
                ).astype(jnp.bfloat16)

    tables = (cos_v, sin_v, inside, query_decay, key_decay)

    def pairs_of(far, i=None):
        project(0, far, i, pairs)

    def values_of(far, i=None):
        project(1, far, i, values)

    def weigh(far):
        loaded(16, 17)
        weigh_blocks(chip_start(far), 2 * rows, tables, pairs, weights, decayed)

    def retain(far):
        loaded(18, 19)
        held = (pairs, weights, decayed, values)
        retain_blocks(chip_start(far), 2 * rows, tables, gain_head, held, memory, head_out)

    lefts, rights = (head_out, hidden), (out_full, down_full)

    def product(layer, taken, rank, place, here):
        for i in range(2):
            start = pl.multiple_of((ga.near(rank) * 2 + i) * cols_of, 128)
            cols = pl.ds(start, cols_of)
            place[here, cols] = jnp.dot(
                lefts[layer][taken, :], rights[layer][:, cols], preferred_element_type=jnp.float32
            ).astype(jnp.bfloat16)

    def rank_joined(layer, rank):
        for far in (0, 1):
            s = (4, 8)[layer] + far
            once(("rank", s, rank), [functools.partial(ga.joined, s, rank)])

    def far_rank(layer, rank, i):
        here, cols = part_rows(i), wide(rank)
        rank_joined(layer, rank)
        if layer == 1:
            swap_far(rank, i).wait_send()
            give(rank, i).wait_send()
        product(layer, far_span(1 - core, i), rank, far_sent, here)
        swap_far(rank, i).start()
        product(layer, far_span(core, i), rank, far_part, here)
        swap_far(rank, i).wait_recv()
        total = far_part[here, cols].astype(jnp.float32) + far_got[here, cols].astype(jnp.float32)
        far_sum[here, cols] = total.astype(jnp.bfloat16)
        give(rank, i).start()

    def own_rank(layer, rank):
        everything = pl.ds(0, rows)
        rank_joined(layer, rank)
        product(layer, chip_rows(0, 1 - core), rank, sent, everything)
        share(rank).start()
        product(layer, chip_rows(0, core), rank, part, everything)

    def norm_mlp(i):
        if i == 0:
            for rank in range(depth):
                share(rank).wait()
        for rank in range(depth):
            give(rank, i).wait_recv()
        join_beside(0, i, 0).wait_send()
        join_own(0, i, core).wait_send()

        @pl.loop(0, splits[i] // ROWS)
        def _(r):
            at = starts[i] + r * ROWS
            here = pl.ds(pl.multiple_of(at, ROWS), ROWS)
            there = pl.ds(pl.multiple_of((y * 2 + core) * rows + at, ROWS), ROWS)
            total = part[here, :].astype(jnp.float32) + got[here, :].astype(jnp.float32)
            total = total + far_in[here, :].astype(jnp.float32)
            mid = (x[here, :].astype(jnp.float32) + total).astype(jnp.bfloat16)
            middle[here, :] = mid
            both[there, :] = scaled_rows(mid.astype(jnp.float32), gain_mlp[...])

        spread(1, i)

    def activate(ranges):
        @pl.loop(0, whole)
        def _(j):
            cols = pl.ds(pl.multiple_of(j * 2 * TILE, 2 * TILE), 2 * TILE)
            place = pl.ds(pl.multiple_of(j * TILE, TILE), TILE)
            for here in ranges:
                two = jnp.dot(both[here, :], gate_up[:, cols], preferred_element_type=jnp.float32)
                hidden[here, place] = (jax.nn.silu(two[:, :TILE]) * two[:, TILE:]).astype(
                    jnp.bfloat16
                )

        half = TILE // 2
        for here in ranges:
            two = jnp.dot(
                both[here, :],
                gate_up[:, pl.ds(2 * aligned, TILE)],
                preferred_element_type=jnp.float32,
            )
            hidden[here, pl.ds(aligned, half)] = (
                jax.nn.silu(two[:, :half]) * two[:, half:]
            ).astype(jnp.bfloat16)

    def expand(far, i=None):
        gathered(3)
        activate(spans(1, far, i))

    def drain():
        for s in range(2 * len(fulls)):
            ga.drain(s)
        for i in range(len(splits)):
            join_own(1, i, core).wait_send()
            join_far(1, i, core).wait_send()
            join_beside(1, i, 0).wait_send()

    def finish():
        drain()
        for rank in range(depth):
            share(rank).wait()
        writes = []
        for i in range(len(splits)):
            here = part_rows(i)
            for rank in range(depth):
                cols = wide(rank)
                give(rank, i).wait_recv()
                total = part[here, cols].astype(jnp.float32) + got[here, cols].astype(jnp.float32)
                total = total + far_in[here, cols].astype(jnp.float32)
                middle[here, cols] = (middle[here, cols].astype(jnp.float32) + total).astype(
                    jnp.bfloat16
                )
                write = pltpu.make_async_copy(
                    middle.at[here, cols], out.at[here, cols], load_sem.at[len(writes)]
                )
                write.start()
                writes.append(write)
        for rank in range(depth):
            for i in range(len(splits)):
                swap_far(rank, i).wait_send()
                give(rank, i).wait_send()
        for write in writes:
            write.wait()

    order = [
        (h, 2, 0), (cross, 1), (h, 0, 0), (cross, 3), (norm_mix,), (cross, 5), (h, 1, 0),
        (h, 2, 1), (h, 0, 1), (h, 1, 1), (h, 2, 2), (h, 0, 2), (cross, 7), (h, 3, 0), (h, 1, 2),
        (cross, 9), (h, 0, 3), (h, 1, 3), (h, 4, 0), (h, 3, 1), (h, 3, 2), (pass_on, 0, 0),
        (h, 2, 3), (h, 6, 0), (h, 3, 3), (pairs_of, 1, 0), (pass_on, 0, 1), (h, 5, 0),
        (pairs_of, 1, 1), (h, 4, 1), (weigh, 1), (values_of, 1, 0), (values_of, 1, 1), (h, 5, 1),
        (retain, 1), (h, 4, 2), (far_rank, 0, 0, 0), (h, 5, 2), (values_of, 0), (h, 7, 0),
        (h, 4, 3), (far_rank, 0, 0, 1), (h, 5, 3), (far_rank, 0, 1, 0), (far_rank, 0, 1, 1),
        (h, 6, 1), (far_rank, 0, 2, 0), (pairs_of, 0), (h, 7, 1), (weigh, 0), (retain, 0),
        (far_rank, 0, 3, 0), (far_rank, 0, 2, 1), (own_rank, 0, 3), (own_rank, 0, 2),
        (far_rank, 0, 3, 1), (h, 6, 2), (own_rank, 0, 1), (own_rank, 0, 0), (norm_mlp, 0),
        (h, 7, 2), (h, 6, 3), (h, 8, 0), (h, 7, 3), (norm_mlp, 1), (h, 9, 0), (pass_on, 1, 0),
        (h, 8, 1), (h, 9, 1), (expand, 1, 0), (h, 8, 2), (far_rank, 1, 0, 0), (pass_on, 1, 1),
        (far_rank, 1, 1, 0), (h, 9, 2), (expand, 1, 1), (far_rank, 1, 0, 1), (far_rank, 1, 1, 1),
        (h, 8, 3), (h, 9, 3), (far_rank, 1, 2, 1), (far_rank, 1, 2, 0), (expand, 0),
        (far_rank, 1, 3, 0), (far_rank, 1, 3, 1), (own_rank, 1, 0), (own_rank, 1, 2),
        (own_rank, 1, 1), (own_rank, 1, 3), (finish,),
    ]
    for job, *given in order:
        job(*given)


def rotation_tables(length_total, half_width):
    position = np.arange(length_total, dtype=np.float32)
    inverse = (1.0 / rope_base ** np.linspace(0.0, 1.0, half_width)).astype(np.float32)
    angle = (position[:, None] * inverse[None, :]).astype(np.float64)
    return np.cos(angle).astype(np.float32), np.sin(angle).astype(np.float32)


def fits(rows, width, key_cols, value_cols, units, shard, out_cols):
    axes = lax.axis_size("rep") == 2 and lax.axis_size("fs") == 8 and lax.axis_size("tp") == 2
    cut = units % (2 * TILE) == TILE and (units // 2) % 32 == 0
    whole = width == 8 * out_cols and width == 8 * shard and shard % 256 == 0
    heads = key_cols == 2 * DK and value_cols == 2 * DV
    return axes and cut and whole and heads and rows % 192 == 0


def layer(args):
    resid, query, gate, down = args[0], args[2], args[8], args[10]
    size = lax.axis_size("fs")
    depth = size // 2
    rows, width = resid.shape
    tokens = 4 * rows
    units = gate.shape[1]
    shard, out_cols = query.shape[0], down.shape[1]
    others = [(shard, 2 * DK), (shard, DV), (DV, out_cols), (shard, units), (units // 2, out_cols)]
    fulls = []
    for (r, c), axis in zip(others, (0, 0, 1, 0, 1)):
        fulls.append((r * size, c) if axis == 0 else (r, c * size))
    along = [shard // 2, shard // 2, DV // 2, shard // 16 * 9 // 16 * 16, units // 2 // 16 * 27 // 44 * 16]
    splits = (2 * rows // 3, rows // 3)
    cosine, sine = rotation_tables(2 * rows, DK // 2)
    far = pl.BlockSpec(memory_space=pl.ANY)
    bf, f32 = jnp.bfloat16, jnp.float32
    vm = pltpu.VMEM
    dma = pltpu.SemaphoreType.DMA
    slices = 2 * len(fulls)
    peers = 2 * len(splits) + (1 + len(splits)) * depth
    args = [a[None, :] if a.ndim == 1 else a for a in args]
    return pl.pallas_call(
        functools.partial(layer_kernel, depth, splits, along),
        out_shape=jax.ShapeDtypeStruct((rows, width), bf),
        in_specs=[far] * 13,
        out_specs=far,
        scratch_shapes=[vm(s, bf) for s in fulls]
        + [vm(s, bf) for s in others]
        + [
            vm((rows, width), bf),
            vm(args[1].shape, f32),
            vm((1, DV), f32),
            vm(args[7].shape, f32),
            vm(cosine.shape, f32),
            vm(sine.shape, f32),
            vm((shard, TILE), bf),
            vm((shard, TILE), bf),
            vm((tokens, width), bf),
            vm((tokens, width), bf),
            vm((tokens, 2 * DK), bf),
            vm((tokens, DV), bf),
            vm((tokens, BLOCK), bf),
            vm((tokens, DK), bf),
            vm((DK, DV), f32),
            vm((tokens, DV), bf),
            vm((tokens, units // 2), bf),
        ]
        + [vm((rows, width), bf)] * 9
        + [vm((BLOCK, BLOCK), f32)] * 3
        + [
            dma((slices, 2 * depth + 1)),
            dma((slices, 2 * depth)),
            dma((len(fulls),)),
            dma((len(fulls),)),
            dma((22,)),
            dma((peers,)),
            dma((peers,)),
            dma((len(splits) * (1 + depth),)),
            dma((len(splits) * (1 + depth),)),
        ],
        compiler_params=pltpu.CompilerParams(
            collective_id=0, has_side_effects=True, vmem_limit_bytes=67043328
        ),
    )(*args, jnp.asarray(cosine), jnp.asarray(sine))


DK = 256
DV = 512
BLOCK = 128


norm_eps = 1e-06
rope_base = 10000.0


def rms_scale(values, gain):
    widened = values.astype(jnp.float32)
    scaled = widened * lax.rsqrt(jnp.mean(widened * widened, axis=-1, keepdims=True) + norm_eps)
    return (scaled * gain).astype(jnp.bfloat16)


def rotation(length_total, half_width):
    position = jnp.arange(length_total, dtype=jnp.float32)
    inverse = 1.0 / rope_base ** jnp.linspace(0.0, 1.0, half_width, dtype=jnp.float32)
    angle = position[:, None] * inverse[None, :]
    return (jnp.cos(angle), jnp.sin(angle))


def rotate(vectors):
    length_total = vectors.shape[0]
    half_width = vectors.shape[-1] // 2
    cosine, sine = rotation(length_total, half_width)
    cosine, sine = cosine[:, None, :], sine[:, None, :]
    first = vectors[..., :half_width]
    second = vectors[..., half_width:]
    return jnp.concatenate(
        [first * cosine - second * sine, second * cosine + first * sine], axis=-1
    )


def decay_tables(head_ids, block):
    log_gamma = jnp.log1p(-(2.0 ** (-5.0 - 2.0 * head_ids.astype(jnp.float32))))
    offset = jnp.arange(block, dtype=jnp.float32)
    distance = offset[:, None] - offset[None, :]
    inside = jnp.where(
        distance >= 0, jnp.exp(log_gamma[:, None, None] * jnp.maximum(distance, 0.0)), 0.0
    )
    query_decay = jnp.exp(log_gamma[:, None] * (offset + 1.0))
    key_decay = jnp.exp(log_gamma[:, None] * (block - 1.0 - offset))
    block_decay = jnp.exp(log_gamma * block)
    return (inside, query_decay, key_decay, block_decay)


def retain(queries, keys, values, head_ids, block):
    length_total, heads, key_width = queries.shape
    value_width = values.shape[-1]
    count = length_total // block
    inside, query_decay, key_decay, block_decay = decay_tables(head_ids, block)

    def blocks(tensor):
        return tensor.reshape(count, block, heads, tensor.shape[-1]).transpose(0, 2, 1, 3)

    def advance(memory, inputs):
        query_tile_rows, key_tile_rows, value_block = inputs
        attention_scores = jnp.einsum(
            "zvf,zjf->zvj", query_tile_rows, key_tile_rows, preferred_element_type=jnp.float32
        )
        weights = (attention_scores * inside).astype(jnp.bfloat16)
        within = jnp.einsum(
            "hlm,hmv->hlv", weights, value_block, preferred_element_type=jnp.float32
        )
        carried = (
            jnp.einsum(
                "hld,hdv->hlv",
                query_tile_rows,
                memory.astype(jnp.bfloat16),
                preferred_element_type=jnp.float32,
            )
            * query_decay[:, :, None]
        )
        weighted_keys = (key_tile_rows.astype(jnp.float32) * key_decay[:, :, None]).astype(
            jnp.bfloat16
        )
        memory = memory * block_decay[:, None, None] + jnp.einsum(
            "hld,hlv->hdv", weighted_keys, value_block, preferred_element_type=jnp.float32
        )
        return (memory, within + carried)

    start_state = jnp.zeros((heads, key_width, value_width), jnp.float32)
    _, outputs = lax.scan(advance, start_state, (blocks(queries), blocks(keys), blocks(values)))
    return outputs.transpose(0, 2, 1, 3).reshape(length_total, heads, value_width)


def head_scale(retained, gain):
    scaled = retained * lax.rsqrt(jnp.mean(retained * retained, axis=-1, keepdims=True) + norm_eps)
    return (scaled.reshape(retained.shape[0], -1) * gain).astype(jnp.bfloat16)


def swap(rows):
    return lax.ppermute(rows, "tp", [(0, 1), (1, 0)])


def join_rows(rows):
    if lax.axis_size("tp") != 2:
        return lax.all_gather(rows, "tp", axis=0, tiled=True)
    first = lax.axis_index("tp") == 0
    got = swap(rows)
    return jnp.concatenate([jnp.where(first, rows, got), jnp.where(first, got, rows)], axis=0)


def share_sum(part):
    if lax.axis_size("tp") != 2:
        summed = lax.psum_scatter(part, "tp", scatter_dimension=0, tiled=True)
        return summed.astype(jnp.float32)
    count = part.shape[0] // 2
    me = lax.axis_index("tp")
    mine = lax.dynamic_slice_in_dim(part, me * count, count, axis=0)
    theirs = lax.dynamic_slice_in_dim(part, (1 - me) * count, count, axis=0)
    return mine.astype(jnp.float32) + swap(theirs).astype(jnp.float32)


def shards(
    resid,
    mix_gain,
    query_weight,
    key_weight,
    value_weight,
    head_gain,
    out_weight,
    mlp_gain,
    gate_weight,
    up_weight,
    down_weight,
):
    token_rows = resid.shape[0]
    length_total = token_rows * lax.axis_size("tp")
    key_cols = query_weight.shape[1]
    heads_here = key_cols // DK
    sizes = (
        token_rows, resid.shape[1], key_cols, value_weight.shape[1], gate_weight.shape[1],
        query_weight.shape[0], down_weight.shape[1],
    )
    if fits(*sizes):
        args = [
            resid, mix_gain, query_weight, key_weight, value_weight, head_gain,
            out_weight, mlp_gain, gate_weight, up_weight, down_weight,
        ]
        return layer(args)
    normed = rms_scale(resid, mix_gain)
    mixer_shard = jnp.concatenate([query_weight, key_weight, value_weight], axis=1)
    mlp_shard = jnp.concatenate([gate_weight, up_weight], axis=1)
    normed_full = join_rows(normed)
    head_ids = lax.axis_index("tp") * heads_here + jnp.arange(heads_here, dtype=jnp.int32)
    pieces = [mixer_shard, out_weight, mlp_shard, down_weight]
    mixer_full, out_full, mlp_full, down_full = (
        lax.all_gather(s, "fs", axis=a, tiled=True) for s, a in zip(pieces, [0, 1, 0, 1])
    )
    projected = jnp.dot(
        normed_full, mixer_full, preferred_element_type=jnp.float32
    ).astype(jnp.bfloat16)
    both_keys = projected[:, : 2 * key_cols].astype(jnp.float32)
    both_keys = both_keys.reshape(length_total, 2, heads_here, DK)
    values = projected[:, 2 * key_cols :].reshape(length_total, heads_here, DV)
    query_rot = rotate(both_keys[:, 0]).astype(jnp.bfloat16)
    key_rot = (rotate(both_keys[:, 1]) * DK ** (-0.5)).astype(jnp.bfloat16)
    retained = retain(query_rot, key_rot, values, head_ids, BLOCK)
    head_out = head_scale(retained, head_gain)
    part = jnp.dot(head_out, out_full, preferred_element_type=jnp.float32).astype(jnp.bfloat16)
    mixer_sum = share_sum(part)
    middle = (resid.astype(jnp.float32) + mixer_sum).astype(jnp.bfloat16)
    normed_mlp = rms_scale(middle, mlp_gain)
    local_units = gate_weight.shape[1]
    both = jnp.dot(
        join_rows(normed_mlp),
        mlp_full,
        preferred_element_type=jnp.float32,
    )
    hidden_units = (jax.nn.silu(both[:, :local_units]) * both[:, local_units:]).astype(jnp.bfloat16)
    mlp_sum = share_sum(
        jnp.dot(hidden_units, down_full, preferred_element_type=jnp.float32).astype(jnp.bfloat16)
    )
    return (middle.astype(jnp.float32) + mlp_sum).astype(jnp.bfloat16)


def solution(mesh):
    placed = (
        P(("rep", "fs", "tp"), None),
        P(),
        P("fs", "tp"),
        P("fs", "tp"),
        P("fs", "tp"),
        P("tp"),
        P("tp", "fs"),
        P(),
        P("fs", "tp"),
        P("fs", "tp"),
        P("tp", "fs"),
    )
    return jax.shard_map(
        shards, mesh=mesh, in_specs=placed, out_specs=P(("rep", "fs", "tp"), None), check_vma=False
    )
```
